512 devices in a mesh: ep: 32 (over z, x), tp: 16 (over y, core).
Axes of the slice: x: 4, y: 8, z: 8, core: 2. Of those that a mesh axis runs over, the one named last changes fastest.
Arguments:
- residual: bfloat16 [256, 2048], P(None, 'ep'), may hold values from -40 to 40
- norm_gain: float32 [2048], P('ep'), may hold values from 0.1 to 1.9
- query_weight: bfloat16 [2048, 2048], P('ep', 'tp'), may hold values from -0.125 to 0.125
- key_weight: bfloat16 [2048, 2048], P('ep', 'tp'), may hold values from -0.125 to 0.125
- value_weight: bfloat16 [2048, 4096], P('ep', 'tp'), may hold values from -0.125 to 0.125
- gate_weight: bfloat16 [2048, 4096], P('ep', 'tp'), may hold values from -0.125 to 0.125
- out_weight: bfloat16 [4096, 2048], P('tp', 'ep'), may hold values from -0.09375 to 0.09375
- prior_state: float32 [256, 16, 128, 256], P('ep', 'tp'), may hold values from -3 to 3
- lengths: int32 [256], P('ep'), may hold values from 1024 to 16383
- ffn_gain: float32 [2048], replicated, may hold values from 0.1 to 1.9
- expert_gate: bfloat16 [32, 2048, 2048], P('ep', None, 'tp'), may hold values from -0.5 to 0.5
- expert_up: bfloat16 [32, 2048, 2048], P('ep', None, 'tp'), may hold values from -0.5 to 0.5
- expert_down: bfloat16 [32, 2048, 2048], P('ep', 'tp'), may hold values from -0.03125 to 0.03125
- route_ids: int32 [256, 4], replicated, may hold values from 0 to 31, all different within a row; in each aligned block of 8 rows (0 to 7, 8 to 15, ...) at most 2 rows name the same one
- route_weight: float32 [256, 4], replicated, may hold values from 0.1 to 1
- dense_gate: bfloat16 [2048, 2048], P('ep', 'tp'), may hold values from -0.125 to 0.125
- dense_up: bfloat16 [2048, 2048], P('ep', 'tp'), may hold values from -0.125 to 0.125
- dense_down: bfloat16 [2048, 2048], P('tp', 'ep'), may hold values from -0.25 to 0.25
- mix_vector: bfloat16 [2048], P('ep'), may hold values from -0.125 to 0.125
Outputs:
- layer_out: bfloat16 [256, 2048], P(None, 'ep')
- new_state: float32 [256, 16, 128, 256], P('ep', 'tp')
The draws below stay inside these ranges and needn't reach their ends.
Inputs may be any that keep to these rules, and one draw needn't show every extreme that they name: `route_ids`: each row names 4 different experts; within each aligned block of 8 rows no expert is named by more than 2 rows, and in some block one expert is named by exactly 2 rows.
All inputs are finite; a program needn't handle non-finite values.
Results may differ from the reference program's by a relative error of at most 0.02.
Values may be sent and summed in bfloat16 or wider, within the bound.
No kernel may reach another device: no remote copies, remote signals or barrier semaphores. Data moves between devices by JAX's collectives and lax.ppermute only.
A program may use at most 64 MiB of HBM per device.

```python
import math
import jax
import jax.numpy as jnp
import numpy as np
from jax import lax

D = 2048
HEADS = 16
KEY_DIM = 128
VAL_DIM = 256
FF = 2048
DENSE = 2048
TOPK = 4
B_DEV = 8
BATCH = 256
EXPERTS = 32
CAP = 2
SLOTS = 64
N_EP = 32
N_TP = 16


def draw_residual(key, part):
    base_key, row_key = jax.random.split(key, 2)
    columns = jnp.arange(D, dtype=jnp.float32) / (D - 1)
    column_scale = 0.35 * jnp.exp(jnp.log(8.0) * columns)
    row_draw = jax.random.uniform(row_key, (BATCH, 1), jnp.float32, 0.0, 1.0)
    row_scale = jnp.exp(jnp.log(10.0) * (row_draw - 0.5))
    base = jax.random.truncated_normal(base_key, -4.0, 4.0, (BATCH, D), jnp.float32)
    return (base * column_scale[None, :] * row_scale).astype(jnp.bfloat16)


def touch_ends(entries, own_key, smallest, largest):
    spot = [jax.random.randint(jax.random.fold_in(own_key, axis), (), 0, length) for axis, length in enumerate(entries.shape)]
    longest = entries.shape.index(max(entries.shape))
    next_to = spot[:longest] + [(spot[longest] + 1) % entries.shape[longest]] + spot[longest + 1:]
    return entries.at[tuple(spot)].set(smallest).at[tuple(next_to)].set(largest)


def with_spikes(array, stream_key, source, target, blocks, factor):
    owner, partner = [(jnp.arange(array.shape[dim]) // (array.shape[dim] // blocks)).reshape([-1 if axis == dim else 1 for axis in range(array.ndim)]) for dim in (source, target)]
    chosen = jax.random.permutation(stream_key, blocks)[partner]
    strong = (owner == chosen) | (owner == (partner + blocks // 2) % blocks)
    return jnp.where(strong, factor * array, array)


def steps_of(rng, shape, cuts, least, largest):
    def one(dim, parts):
        heights = jax.random.uniform(jax.random.fold_in(jax.random.fold_in(rng, 6), dim), (parts,), jnp.float32, least / len(cuts), largest / len(cuts))
        return jnp.repeat(jnp.exp(heights), shape[dim] // parts).reshape((-1,) + (1,) * (len(shape) - dim - 1))

    loudness = one(*cuts[0])
    for cut in cuts[1:]:
        loudness = loudness * one(*cut)
    return loudness


def deal_out(own_key, own, number, rows, amount, top, most, lean):
    ranking = jax.random.permutation(own_key, amount)
    crowded, ordinary = shares(amount, rows * top, most, lean, True), shares(amount, rows * top, most, lean, False)
    places = jnp.arange(amount)

    def named(sizes, turn):
        used = int((sizes > 0).sum())
        fixed = max(1, used // 4)
        passed = fixed + (places - fixed + turn * (used - fixed)) % max(1, amount - fixed)
        return jnp.zeros((amount,), jnp.int32).at[ranking[jnp.where(places < fixed, places, passed)]].set(jnp.asarray(sizes, jnp.int32))

    sizes = jnp.where(number % 4 == 0, named(crowded, number // 4), named(ordinary, number - number // 4 - 1))
    mixed = jax.random.permutation(jax.random.fold_in(own, 3), amount)
    source_of, receiver = mixed[0:amount // 2 * 2:2], mixed[1:amount // 2 * 2:2]
    room = jnp.minimum(sizes[source_of] - 1, most - sizes[receiver]) // 2
    room = jnp.where((source_of == ranking[0]) | (receiver == ranking[0]) | (sizes[receiver] == 0), 0, jnp.maximum(room, 0))
    passed = jax.random.randint(jax.random.fold_in(own, 4), (amount // 2,), 0, 1 << 20) % (room + 1)
    sizes = sizes.at[source_of].add(-passed).at[receiver].add(passed)
    members = jnp.searchsorted(jnp.cumsum(sizes), jnp.arange(rows * top), side="right").astype(jnp.int32)
    grid = members.reshape(top, rows).T
    grid = grid[jax.random.permutation(jax.random.fold_in(own, 1), rows)]
    turn = jax.random.randint(jax.random.fold_in(own, 2), (rows, 1), 0, top)
    return jnp.take_along_axis(grid, (jnp.arange(top)[None, :] + turn) % top, axis=1)


def shares(amount, total, most, lean, full):
    loads = [(1 << 20) // math.isqrt(rank ** lean) + 1 for rank in range(1, amount + 1)]
    largest = most if full else min(most, max(-(-total // amount), total * loads[0] // sum(loads)))
    least = 1 if total - largest >= amount - 1 else 0
    holding, rest = [largest] + [least] * (amount - 1), total - largest - least * (amount - 1)
    while rest > 0:
        movable = [i for i in range(1, amount) if holding[i] < largest] or [i for i in range(1, amount) if holding[i] < most]
        whole, left = sum([loads[i] for i in movable]), rest
        for i in movable:
            addition = min(most - holding[i], max(1, left * loads[i] // whole), rest)
            holding[i] = holding[i] + addition
            rest = rest - addition
    return np.array(holding)


def noise(own_key, extent, scale, reach, cuts=(), kind=jnp.bfloat16):
    values = scale * jax.random.normal(own_key, extent, jnp.float32)
    if cuts:
        values = values * steps_of(own_key, extent, cuts, -0.22, 0.18)
    return jnp.clip(values, -reach, reach).astype(kind)


def noise_with(own_key, dims, scale, most, shards, heavy, kind=jnp.bfloat16):
    entries = scale * jax.random.normal(own_key, dims, jnp.float32)
    if shards:
        entries = entries * steps_of(own_key, dims, shards, -0.22, 0.18)
    return jnp.clip(with_spikes(entries, jax.random.fold_in(own_key, 3), *heavy), -most, most).astype(kind)


def setup_inputs(seed: int = 0) -> dict:
    splits = jax.random.split(jax.random.key(seed), 20)
    residual = draw_residual(jax.random.fold_in(splits[19], 71), 0)
    norm_gain = jnp.clip(1.0 + 0.18 * jax.random.normal(splits[1], (D,), jnp.float32), 0.1, 1.9)
    query_weight = noise(splits[2], (D, HEADS * KEY_DIM), D ** -0.5, 0.125, ((0, 32), (1, 16)))
    key_weight = noise(splits[3], (D, HEADS * KEY_DIM), D ** -0.5, 0.125, ((0, 32), (1, 16)))
    value_weight = noise(splits[4], (D, HEADS * VAL_DIM), D ** -0.5, 0.125, ((0, 32), (1, 16)))
    gate_weight = noise(splits[5], (D, HEADS * VAL_DIM), D ** -0.5, 0.125, ((0, 32), (1, 16)))
    out_weight = noise(splits[6], (HEADS * VAL_DIM, D), (HEADS * VAL_DIM) ** -0.5, 0.09375, ((0, 16), (1, 32)))
    prior_state = noise(splits[7], (BATCH, HEADS, KEY_DIM, VAL_DIM), 0.5, 3.0, ((0, 32), (1, 16)), jnp.float32)
    lengths = touch_ends(jax.random.randint(splits[8], (BATCH,), 1024, 16384), jax.random.fold_in(splits[8], 1), 1024, 16383).astype(jnp.int32)
    ffn_gain = jnp.clip(1.0 + 0.18 * jax.random.normal(splits[9], (D,), jnp.float32), 0.1, 1.9)
    expert_gate = noise(splits[10], (EXPERTS, D, FF), (D // 16) ** -0.5, 0.5, ((0, 32), (2, 16)))
    expert_up = noise(splits[11], (EXPERTS, D, FF), (D // 16) ** -0.5, 0.5, ((0, 32), (2, 16)))
    expert_down = noise(splits[12], (EXPERTS, FF, D), (FF * 16) ** -0.5, 0.03125, ((0, 32), (1, 16)))
    route_ids_keys = jax.random.split(jax.random.fold_in(splits[13], 1), BATCH // B_DEV)
    route_ids_turns = jax.random.permutation(jax.random.fold_in(splits[13], 3), BATCH // B_DEV)
    route_ids = jax.vmap(lambda own, number: deal_out(jax.random.fold_in(splits[13], 2), own, number, B_DEV, EXPERTS, TOPK, CAP, 2))(route_ids_keys, route_ids_turns).reshape((BATCH, TOPK))
    route_weight = jnp.clip(jnp.exp(jax.random.uniform(splits[14], (BATCH, TOPK), jnp.float32, math.log(0.1), math.log(1.0))), 0.1, 1.0)
    dense_gate = noise(splits[15], (D, DENSE), D ** -0.5, 0.125, ((0, 32), (1, 16)))
    dense_up = noise(splits[16], (D, DENSE), D ** -0.5, 0.125, ((0, 32), (1, 16)))
    dense_down = noise_with(splits[17], (DENSE, D), DENSE ** -0.5, 0.25, ((0, 16), (1, 32)), (0, 1, 32, 2.75))
    mix_vector = noise(splits[18], (D,), D ** -0.5, 0.125, ((0, 32),))
    return {"residual": residual, "norm_gain": norm_gain, "query_weight": query_weight, "key_weight": key_weight, "value_weight": value_weight, "gate_weight": gate_weight, "out_weight": out_weight, "prior_state": prior_state, "lengths": lengths, "ffn_gain": ffn_gain, "expert_gate": expert_gate, "expert_up": expert_up, "expert_down": expert_down, "route_ids": route_ids, "route_weight": route_weight, "dense_gate": dense_gate, "dense_up": dense_up, "dense_down": dense_down, "mix_vector": mix_vector}


norm_eps = 1e-06
clamp_limit = 7.0
gate_alpha = 1.702

def rotate_half(vectors, positions):
    half_dim = vectors.shape[-1] // 2
    inverse = 1.0 / 10000.0 ** jnp.linspace(0.0, 1.0, half_dim, dtype=jnp.float32)
    angles = positions.astype(jnp.float32)[:, None] * inverse[None, :]
    cosine = jnp.cos(angles)[:, None, :]
    sine_part = jnp.sin(angles)[:, None, :]
    first_half = vectors[..., :half_dim]
    second_half = vectors[..., half_dim:]
    return jnp.concatenate([first_half * cosine - second_half * sine_part, second_half * cosine + first_half * sine_part], axis=-1)

def grouped_product(left_rows, right_rows, groups):
    block_width = left_rows.shape[1] // groups
    left_blocks = left_rows.reshape(left_rows.shape[0], groups, block_width).astype(jnp.float32)
    right_blocks = right_rows.reshape(groups, block_width, right_rows.shape[1]).astype(jnp.float32)
    partial_value = jnp.einsum('bgw,gwd->gbd', left_blocks, right_blocks)
    rounded = lax.optimization_barrier(partial_value.astype(jnp.bfloat16))
    return lax.optimization_barrier(jnp.sum(rounded.astype(jnp.float32), axis=0))

def slot_index(route_ids, groups, capacity, experts):
    pair_ids = route_ids.reshape(groups, -1)
    labels = jnp.arange(experts, dtype=jnp.int32)
    onehot = (pair_ids[:, :, None] == labels[None, None, :]).astype(jnp.int32)
    earlier = jnp.cumsum(onehot, axis=1) - onehot
    within = lax.optimization_barrier(jnp.sum(earlier * onehot, axis=2))
    offset = jnp.arange(groups, dtype=jnp.int32)[:, None] * capacity
    return (pair_ids * (groups * capacity) + offset + within).reshape(-1).astype(jnp.int32)

def source_rows(target, total_rows, topk_count, table_size):
    owners = jnp.arange(target.shape[0], dtype=jnp.int32) // topk_count
    return jnp.full((table_size,), total_rows, jnp.int32).at[target].set(owners)

def expert_block(rows_in, gain, gate_w, up_w, down_w, groups):
    rows_float = rows_in.astype(jnp.float32)
    row_norm = lax.rsqrt(lax.optimization_barrier(jnp.mean(rows_float * rows_float, axis=1, keepdims=True)) + norm_eps)
    normed = (rows_float * gain).astype(jnp.bfloat16)
    gate_val = jnp.minimum(jnp.dot(normed, gate_w, preferred_element_type=jnp.float32) * row_norm, clamp_limit)
    up_val = jnp.clip(jnp.dot(normed, up_w, preferred_element_type=jnp.float32) * row_norm, -clamp_limit, clamp_limit)
    hidden = ((up_val + 1.0) * gate_val * jax.nn.sigmoid(gate_alpha * gate_val)).astype(jnp.bfloat16)
    return grouped_product(hidden, down_w, groups).astype(jnp.bfloat16)

def reference(residual, norm_gain, query_weight, key_weight, value_weight, gate_weight, out_weight, prior_state, lengths, ffn_gain, expert_gate, expert_up, expert_down, route_ids, route_weight, dense_gate, dense_up, dense_down, mix_vector):
    batch_rows = residual.shape[0]
    residual_float = residual.astype(jnp.float32)
    row_scale = lax.rsqrt(lax.optimization_barrier(jnp.mean(residual_float * residual_float, axis=1, keepdims=True)) + norm_eps)
    normed_in = (residual_float * norm_gain).astype(jnp.bfloat16)
    query = jnp.dot(normed_in, query_weight, preferred_element_type=jnp.float32) * row_scale
    key_raw = jnp.dot(normed_in, key_weight, preferred_element_type=jnp.float32) * row_scale
    value_proj = jnp.dot(normed_in, value_weight, preferred_element_type=jnp.float32) * row_scale
    gate_pre = jnp.dot(normed_in, gate_weight, preferred_element_type=jnp.float32) * row_scale
    query_rot = rotate_half(query.reshape(batch_rows, HEADS, KEY_DIM), lengths)
    key_rot = rotate_half(key_raw.reshape(batch_rows, HEADS, KEY_DIM), lengths) * KEY_DIM ** (-0.5)
    values = value_proj.reshape(batch_rows, HEADS, VAL_DIM)
    decay_rate = 1.0 - jnp.exp2(-1.0 - 0.5 * jnp.arange(HEADS, dtype=jnp.float32))
    new_state = decay_rate[None, :, None, None] * prior_state + key_rot[:, :, :, None] * values[:, :, None, :]
    state_read = jnp.einsum('bhk,bhkv->bhv', query_rot, new_state, precision=lax.Precision.HIGHEST)
    normed = state_read * lax.rsqrt(lax.optimization_barrier(jnp.mean(state_read * state_read, axis=-1, keepdims=True)) + norm_eps)
    gated_out = (normed * jax.nn.silu(gate_pre.reshape(batch_rows, HEADS, VAL_DIM))).astype(jnp.bfloat16)
    gated_out = gated_out.reshape(batch_rows, HEADS * VAL_DIM)
    attn_out = grouped_product(gated_out, out_weight, N_TP)
    after_mixer = (residual_float + attn_out).astype(jnp.bfloat16)
    target = slot_index(route_ids, N_EP, CAP, EXPERTS)
    slot_source = source_rows(target, batch_rows, TOPK, EXPERTS * SLOTS)
    padded = jnp.concatenate([after_mixer, jnp.zeros((1, D), jnp.bfloat16)], axis=0)
    expert_in = padded[slot_source].reshape(EXPERTS, SLOTS, D)

    def run_expert(operands):
        rows_in, gate_w, up_w, down_w = operands
        return expert_block(rows_in, ffn_gain, gate_w, up_w, down_w, N_TP)
    expert_out = lax.map(run_expert, (expert_in, expert_gate, expert_up, expert_down))
    picked = expert_out.reshape(EXPERTS * SLOTS, D)[target].reshape(batch_rows, TOPK, D).astype(jnp.float32)
    routed = lax.optimization_barrier(jnp.sum(picked * route_weight[:, :, None], axis=1))
    after_float = after_mixer.astype(jnp.float32)
    ffn_scale = lax.rsqrt(lax.optimization_barrier(jnp.mean(after_float * after_float, axis=1, keepdims=True)) + norm_eps)
    normed_ffn = (after_float * ffn_gain).astype(jnp.bfloat16)
    dense_g = jnp.dot(normed_ffn, dense_gate, preferred_element_type=jnp.float32) * ffn_scale
    dense_u = jnp.dot(normed_ffn, dense_up, preferred_element_type=jnp.float32) * ffn_scale
    dense_act = (jax.nn.silu(dense_g) * dense_u).astype(jnp.bfloat16)
    dense_out = grouped_product(dense_act, dense_down, N_TP)
    mix_logit = jnp.dot(normed_ffn, mix_vector, preferred_element_type=jnp.float32)
    dense_mix = jax.nn.sigmoid(ffn_scale[:, 0] * mix_logit)
    layer_out = (after_float + routed + dense_mix[:, None] * dense_out).astype(jnp.bfloat16)
    return (layer_out, new_state)
```

```python
import functools

import jax
import jax.numpy as jnp
from jax import lax
from jax.experimental import pallas as pl
from jax.experimental.pallas import tpu as pltpu
from jax.sharding import Mesh, PartitionSpec as P

D = 2048
KEY_DIM = 128
VAL_DIM = 256
EPS = 1e-06
LIMIT = 7.0
ALPHA = 1.702
F32 = jnp.float32
BF16 = jnp.bfloat16
EP = ("z", "x")


def mm(a, b):
    return jnp.dot(a, b, preferred_element_type=F32)


def two_part(v):
    high = v.astype(BF16).astype(F32)
    return high, v - high


def lane_of(shape):
    return lax.broadcasted_iota(jnp.int32, shape, len(shape) - 1)


def project_body(res_ref, gain_ref, q_ref, k_ref, v_ref, g_ref, out_ref):
    rows = res_ref[...].astype(F32)
    normed = (rows * gain_ref[...]).astype(BF16)
    at = 0
    for ref in (q_ref, k_ref, v_ref, g_ref):
        width = ref.shape[1]
        part = mm(normed, ref[...])
        out_ref[:, :, at : at + width] = part.reshape(32, 8, width).astype(BF16)
        at += width
    high, low = two_part(jnp.sum(rows * rows, axis=1, keepdims=True))
    lane = lane_of((256, 128))
    stats = jnp.where(lane == 0, high, jnp.where(lane == 1, low, 0.0))
    out_ref[:, :, at : at + 128] = stats.reshape(32, 8, 128).astype(BF16)


def dispatch_body(am_ref, sel_ref, gain_ref, mix_ref, dw_ref, out_ref):
    am = am_ref[...]
    lane = lane_of(am.shape)
    left = lane < 64
    amf = am.astype(F32)
    stacked = jnp.concatenate([jnp.where(left, amf, 0.0), jnp.where(left, 0.0, amf)], axis=0)
    sent = mm(sel_ref[...], stacked.astype(BF16))
    out_ref[:, 0:32, :] = sent.reshape(32, 32, 128).astype(BF16)
    normed = (stacked * gain_ref[...]).astype(BF16)
    both = mm(normed, dw_ref[...])
    out_ref[:, 32:40, :] = both[:, :128].reshape(32, 8, 128).astype(BF16)
    out_ref[:, 40:48, :] = both[:, 128:].reshape(32, 8, 128).astype(BF16)
    sq_high, sq_low = two_part(jnp.sum(stacked * stacked, axis=1, keepdims=True))
    mx_high, mx_low = two_part(
        jnp.sum(normed.astype(F32) * mix_ref[...], axis=1, keepdims=True)
    )
    lane2 = lane_of((256, 128))
    stats = jnp.where(
        lane2 == 0,
        sq_high,
        jnp.where(
            lane2 == 1, sq_low, jnp.where(lane2 == 2, mx_high, jnp.where(lane2 == 3, mx_low, 0.0))
        ),
    )
    out_ref[:, 48:56, :] = stats.reshape(32, 8, 128).astype(BF16)


def expert_body(arr_ref, gain_ref, eg_ref, eu_ref, ed_ref, weight_ref, out_ref, zn_ref):
    tail = jnp.sum(arr_ref[:, 32:56, :].astype(F32), axis=0)
    stats = tail[16:24]
    scale = lax.rsqrt((stats[:, 0:1] + stats[:, 1:2]) / D + EPS)
    mix = jax.nn.sigmoid(scale * (stats[:, 2:3] + stats[:, 3:4]))
    act = jax.nn.silu(tail[0:8] * scale) * (tail[8:16] * scale) * mix
    out_ref[:, 32:40, :] = jnp.broadcast_to(act[None], (32, 8, 128)).astype(BF16)
    left = lane_of((32, 128)) < 64
    squares = jnp.zeros((64, 128), F32)
    for p in range(16):
        a = arr_ref[2 * p, 0:32, :].astype(F32)
        b = arr_ref[2 * p + 1, 0:32, :].astype(F32)
        z = jnp.concatenate(
            [
                jnp.where(left, a, pltpu.roll(b, 64, 1)),
                jnp.where(left, pltpu.roll(a, 64, 1), b),
            ],
            axis=0,
        )
        squares = squares + z * z
        zn_ref[:, 128 * p : 128 * p + 128] = (
            z * gain_ref[:, 128 * p : 128 * p + 128]
        ).astype(BF16)
    norm = lax.rsqrt(jnp.sum(squares, axis=1, keepdims=True) / D + EPS)
    zn = zn_ref[...]
    gate = jnp.minimum(mm(zn, eg_ref[...]) * norm, LIMIT)
    up = jnp.clip(mm(zn, eu_ref[...]) * norm, -LIMIT, LIMIT)
    hidden = ((up + 1.0) * gate * jax.nn.sigmoid(ALPHA * gate)).astype(BF16)
    weight = weight_ref[...]
    for p in range(16):
        o = mm(hidden, ed_ref[:, 128 * p : 128 * p + 128]) * weight
        low, high = o[0:32], o[32:64]
        out_ref[2 * p, 0:32, :] = jnp.where(left, low, pltpu.roll(high, 64, 1)).astype(BF16)
        out_ref[2 * p + 1, 0:32, :] = jnp.where(left, pltpu.roll(low, 64, 1), high).astype(BF16)


def collect_body(arr_ref, low_ref, high_ref, dd_ref, out_ref):
    slots = arr_ref[:, 0:32, :].reshape(1024, 128)
    left = lane_of((128, 128)) < 64
    routed = jnp.where(left, mm(low_ref[...], slots), mm(high_ref[...], slots))
    act = arr_ref[:, 32:40, :].astype(F32).reshape(256, 128).astype(BF16)
    dense = mm(act[:128], dd_ref[0:128]) + mm(act[128:], dd_ref[128:256])
    out_ref[...] = (routed + dense).astype(BF16)


def call(body, out_shape, *args, scratch=()):
    return pl.pallas_call(
        body,
        out_shape=jax.ShapeDtypeStruct(out_shape, BF16),
        in_specs=[pl.BlockSpec(memory_space=pltpu.VMEM)] * len(args),
        out_specs=pl.BlockSpec(memory_space=pltpu.VMEM),
        scratch_shapes=list(scratch),
        name=body.__name__,
    )(*args)


def exchange(pieces, axes):
    return lax.all_to_all(pieces, axes, 0, 0, tiled=True)


def from_everyone(value, axes):
    peers = lax.axis_size(axes)
    return exchange(jnp.broadcast_to(value[None], (peers, *value.shape)), axes)


def own_half(value, core):
    rows = value.shape[0] // 2
    return lax.dynamic_slice_in_dim(value, core * rows, rows, 0)


def half_sum(partial, core):
    both = lax.all_gather(partial, "c")
    mine = lax.dynamic_slice_in_dim(both, core * 64, 64, 1).astype(F32)
    pair = (mine[0] + mine[1]).astype(BF16)
    return jnp.sum(from_everyone(pair, ("y",)).astype(F32), axis=0)


def packed(value):
    rows = value.shape[0] // 2
    return jnp.concatenate([value[:rows], value[rows:]], axis=1)


def block_pair(w):
    zero = jnp.zeros_like(w)
    return jnp.concatenate(
        [jnp.concatenate([w, zero], axis=1), jnp.concatenate([zero, w], axis=1)], axis=0
    )


def rotate_half(vectors, cosine, sine):
    a = vectors[:, :64]
    b = vectors[:, 64:]
    return jnp.concatenate([a * cosine - b * sine, b * cosine + a * sine], axis=1)


def routing(route_ids, route_weight, own):
    rows = route_ids.shape[0]
    names = jnp.arange(32, dtype=jnp.int32)
    hit = route_ids[:, :, None] == names[None, None, :]
    named = jnp.any(hit, axis=1)
    weight = jnp.sum(jnp.where(hit, route_weight[:, :, None], 0.0), axis=1)
    r = lax.broadcasted_iota(jnp.int32, (rows, rows), 0)
    q = lax.broadcasted_iota(jnp.int32, (rows, rows), 1)
    before = ((r // 8 == q // 8) & (q < r)).astype(BF16)
    earlier = mm(before, named.astype(BF16))
    group = lax.broadcasted_iota(jnp.int32, (rows, 1), 0) // 8
    place = ((group % 16) * 2).astype(F32) + earlier
    place = jnp.where(named, place, 64.0).astype(BF16)
    x = lax.broadcasted_iota(jnp.int32, (32, 1024), 0)
    slot = lax.broadcasted_iota(jnp.int32, (32, 1024), 1)
    spread = (slot // 32 == x).astype(BF16)
    wide = mm(place, spread)
    step = (lax.broadcasted_iota(jnp.int32, (1, 1024), 1) % 32).astype(F32)
    back = (wide == step).astype(BF16)
    tall = lax.dot_general(spread, place, (((0,), (1,)), ((), ())), preferred_element_type=F32)
    down = (lax.broadcasted_iota(jnp.int32, (1024, 1), 0) % 32).astype(F32)
    forth = (tall == down).astype(BF16)
    mine = lax.dynamic_slice_in_dim(forth, own * 32, 32, 0).astype(F32)
    own_weight = lax.dynamic_slice_in_dim(weight, own, 1, 1).reshape(1, rows)
    scaled = mine * own_weight
    slot_weight = jnp.concatenate(
        [
            jnp.sum(scaled[:, :128], axis=1, keepdims=True),
            jnp.sum(scaled[:, 128:], axis=1, keepdims=True),
        ],
        axis=0,
    )
    return forth, back[:128], back[128:], jnp.broadcast_to(slot_weight, (64, 128))


def per_device(
    residual,
    norm_gain,
    query_weight,
    key_weight,
    value_weight,
    gate_weight,
    out_weight,
    prior_state,
    lengths,
    ffn_gain,
    expert_gate,
    expert_up,
    expert_down,
    route_ids,
    route_weight,
    dense_gate,
    dense_up,
    dense_down,
    mix_vector,
):
    own = lax.axis_index(EP)
    core = lax.axis_index("c")
    head = lax.axis_index("y") * 2 + core
    terms = call(
        project_body,
        (32, 8, 896),
        residual,
        norm_gain[None, :],
        query_weight,
        key_weight,
        value_weight,
        gate_weight,
    )
    arrived = exchange(terms, EP)

    forth, back_low, back_high, slot_weight = routing(route_ids, route_weight, own)
    out_pair = block_pair(out_weight)
    down_pair = block_pair(dense_down)
    gain_here = lax.dynamic_slice_in_dim(ffn_gain, own * 64, 64, 0)
    gain_pair = jnp.concatenate([gain_here, gain_here])[None, :]
    mix_pair = jnp.concatenate([mix_vector, mix_vector]).astype(F32)[None, :]
    dense_in = jnp.concatenate([dense_gate, dense_up], axis=1)
    dense_in = jnp.concatenate([dense_in, dense_in], axis=0)
    residual_half = own_half(packed(residual), core).astype(F32)
    inverse = 1.0 / 10000.0 ** jnp.linspace(0.0, 1.0, 64, dtype=F32)
    angles = lengths.astype(F32)[:, None] * inverse[None, :]
    cosine = jnp.cos(angles)
    sine = jnp.sin(angles)

    summed = jnp.sum(arrived.astype(F32), axis=0)
    row_scale = lax.rsqrt((summed[:, 768:769] + summed[:, 769:770]) / D + EPS)
    projected = summed[:, :768] * row_scale
    query_rot = rotate_half(projected[:, :128], cosine, sine)
    key_rot = rotate_half(projected[:, 128:256], cosine, sine) * KEY_DIM ** (-0.5)
    values = projected[:, 256:512]
    gate_pre = projected[:, 512:768]
    decay = 1.0 - jnp.exp2(-1.0 - 0.5 * head.astype(F32))
    new_state = decay * prior_state + key_rot[:, None, :, None] * values[:, None, None, :]
    read = jnp.sum(query_rot[:, :, None] * new_state[:, 0], axis=1)
    normed = read * lax.rsqrt(jnp.mean(read * read, axis=-1, keepdims=True) + EPS)
    gated = (normed * jax.nn.silu(gate_pre)).astype(BF16)

    heads = from_everyone(gated, EP).reshape(256, VAL_DIM)
    attn = mm(packed(heads), out_pair).astype(BF16)
    after_half = (residual_half + half_sum(attn, core)).astype(BF16)
    after = lax.all_gather(after_half, "c", tiled=True)

    sent = call(dispatch_body, (32, 56, 128), after, forth, gain_pair, mix_pair, dense_in)
    inbox = exchange(sent, EP)
    made = call(
        expert_body,
        (32, 40, 128),
        inbox,
        ffn_gain[None, :],
        expert_gate[0],
        expert_up[0],
        expert_down[0],
        slot_weight,
        scratch=(pltpu.VMEM((64, D), BF16),),
    )
    returned = exchange(made, EP)
    branch = call(collect_body, (128, 128), returned, back_low, back_high, down_pair)
    out_half = (after_half.astype(F32) + half_sum(branch, core)).astype(BF16)
    out = lax.all_gather(out_half, "c", tiled=True)
    layer_out = jnp.concatenate([out[:, :64], out[:, 64:]], axis=0)
    return layer_out, new_state


def solution(mesh):
    fine = Mesh(mesh.devices.reshape(8, 4, 8, 2), ("z", "x", "y", "c"))
    tp = ("y", "c")
    placed = (
        P(None, EP),
        P(EP),
        P(EP, tp),
        P(EP, tp),
        P(EP, tp),
        P(EP, tp),
        P(tp, EP),
        P(EP, tp, None, None),
        P(EP),
        P(),
        P(EP, None, tp),
        P(EP, None, tp),
        P(EP, tp, None),
        P(),
        P(),
        P(EP, tp),
        P(EP, tp),
        P(tp, EP),
        P(EP),
    )
    return jax.shard_map(
        per_device,
        mesh=fine,
        in_specs=placed,
        out_specs=(P(None, EP), P(EP, tp, None, None)),
        check_vma=False,
    )
```

```python
import jax
import jax.numpy as jnp
from jax import lax
from jax.experimental import pallas as pl
from jax.experimental.pallas import tpu as pltpu
from jax.sharding import Mesh, PartitionSpec as P

D = 2048
KEY_DIM = 128
VAL_DIM = 256
EPS = 1e-06
LIMIT = 7.0
ALPHA = 1.702
F32 = jnp.float32
BF16 = jnp.bfloat16
EP = ("z", "x")


def mm(a, b):
    return jnp.dot(a, b, preferred_element_type=F32)


def dots(a, b, i, j):
    return lax.dot_general(a, b, (((i,), (j,)), ((), ())), preferred_element_type=F32)


def two_part(v):
    high = v.astype(BF16).astype(F32)
    return high, v - high


def lane_of(shape):
    return lax.broadcasted_iota(jnp.int32, shape, len(shape) - 1)


def project_body(res_ref, gain_ref, q_ref, k_ref, v_ref, g_ref, out_ref):
    rows = res_ref[...].astype(F32).T
    normed = (rows * gain_ref[...]).astype(BF16)
    at = 0
    for ref in (q_ref, k_ref, v_ref, g_ref):
        width = ref.shape[1]
        part = mm(normed, ref[...])
        out_ref[:, :, at : at + width] = part.reshape(32, 8, width).astype(BF16)
        at += width
    high, low = two_part(jnp.sum(rows * rows, axis=1, keepdims=True))
    lane = lane_of((256, 128))
    stats = jnp.where(lane == 0, high, jnp.where(lane == 1, low, 0.0))
    out_ref[:, :, at : at + 128] = stats.reshape(32, 8, 128).astype(BF16)


def retain_body(arr_ref, prior_ref, cos_ref, sin_ref, decay_ref, out_ref, key_ref, value_ref):
    summed = jnp.sum(arr_ref[...].astype(F32), axis=0)
    scale = lax.rsqrt((summed[:, 768:769] + summed[:, 769:770]) / D + EPS)
    cosine = cos_ref[...]
    sine = sin_ref[...]
    query = summed[:, 0:128] * scale
    query = query * cosine + pltpu.roll(query, 64, 1) * sine
    key = summed[:, 128:256] * scale
    key = (key * cosine + pltpu.roll(key, 64, 1) * sine) * KEY_DIM ** (-0.5)
    value = summed[:, 256:512] * scale
    gate = summed[:, 512:768] * scale
    key_ref[...] = key
    value_ref[...] = value
    turned = query.T
    reads = [
        jnp.sum(turned[:, b : b + 1] * prior_ref[b], axis=0, keepdims=True) for b in range(8)
    ]
    met = jnp.sum(query * key, axis=1, keepdims=True)
    read = decay_ref[...] * jnp.concatenate(reads, axis=0) + met * value
    normed = read * lax.rsqrt(jnp.mean(read * read, axis=1, keepdims=True) + EPS)
    gated = normed * jax.nn.silu(gate)
    out_ref[...] = jnp.broadcast_to(gated[None], (32, 8, VAL_DIM)).astype(BF16)


def dispatch_body(am_ref, sel_ref, gain_ref, dw_ref, out_ref):
    am = am_ref[...]
    none = jnp.zeros((64, 128), BF16)
    stacked = jnp.concatenate(
        [
            jnp.concatenate([am[:, :128], none], axis=1),
            jnp.concatenate([none, am[:, 128:]], axis=1),
        ],
        axis=0,
    )
    sent = dots(sel_ref[...], stacked, 1, 1)
    out_ref[:, 0:32, :] = sent.reshape(32, 32, 128).astype(BF16)
    amf = am.astype(F32)
    normed = (amf * gain_ref[:, 0:1]).astype(BF16)
    both = dots(normed, dw_ref[...], 0, 0)
    out_ref[:, 32:40, :] = both[:, :128].reshape(32, 8, 128).astype(BF16)
    out_ref[:, 40:48, :] = both[:, 128:256].reshape(32, 8, 128).astype(BF16)
    high, low = two_part(amf * amf)
    squares = jnp.concatenate([high, low], axis=0).astype(BF16)
    second = (lane_of((128, 128)) == 1).astype(F32).astype(BF16)
    stats = both[:, 256:384] + dots(squares, second, 0, 0)
    high, low = two_part(stats)
    stats = high + pltpu.roll(low, 2, 1)
    out_ref[:, 48:56, :] = stats.reshape(32, 8, 128).astype(BF16)


def expert_body(arr_ref, gain_ref, eg_ref, eu_ref, ed_ref, weight_ref, out_ref, zn_ref):
    tail = jnp.sum(arr_ref[:, 32:56, :].astype(F32), axis=0)
    stats = tail[16:24]
    scale = lax.rsqrt((stats[:, 1:2] + stats[:, 3:4]) / D + EPS)
    mix = jax.nn.sigmoid(scale * (stats[:, 0:1] + stats[:, 2:3]))
    act = jax.nn.silu(tail[0:8] * scale) * (tail[8:16] * scale) * mix
    out_ref[:, 32:40, :] = jnp.broadcast_to(act[None], (32, 8, 128)).astype(BF16)
    left = lane_of((32, 128)) < 64
    squares = jnp.zeros((64, 128), F32)
    for p in range(16):
        a = arr_ref[2 * p, 0:32, :].astype(F32)
        b = arr_ref[2 * p + 1, 0:32, :].astype(F32)
        z = jnp.concatenate(
            [
                jnp.where(left, a, pltpu.roll(b, 64, 1)),
                jnp.where(left, pltpu.roll(a, 64, 1), b),
            ],
            axis=0,
        )
        squares = squares + z * z
        zn_ref[:, 128 * p : 128 * p + 128] = (
            z * gain_ref[:, 128 * p : 128 * p + 128]
        ).astype(BF16)
    norm = lax.rsqrt(jnp.sum(squares, axis=1, keepdims=True) / D + EPS)
    zn = zn_ref[...]
    gate = jnp.minimum(mm(zn, eg_ref[...]) * norm, LIMIT)
    up = jnp.clip(mm(zn, eu_ref[...]) * norm, -LIMIT, LIMIT)
    hidden = ((up + 1.0) * gate * jax.nn.sigmoid(ALPHA * gate)).astype(BF16)
    weight = weight_ref[...]
    for p in range(16):
        o = mm(hidden, ed_ref[:, 128 * p : 128 * p + 128]) * weight
        low, high = o[0:32], o[32:64]
        out_ref[2 * p, 0:32, :] = jnp.where(left, low, pltpu.roll(high, 64, 1)).astype(BF16)
        out_ref[2 * p + 1, 0:32, :] = jnp.where(left, pltpu.roll(low, 64, 1), high).astype(BF16)


def collect_body(arr_ref, sel_ref, dd_ref, out_ref):
    slots = arr_ref[:, 0:32, :].reshape(1024, 128)
    both = dots(slots, sel_ref[...], 0, 0)
    act = arr_ref[:, 32:40, :].astype(F32).reshape(256, 128).astype(BF16)
    dense = dots(dd_ref[...], act, 1, 1)
    out_ref[:, :128] = (both[:64, :128] + dense[:, :128]).astype(BF16)
    out_ref[:, 128:] = (both[64:, 128:] + dense[:, 128:]).astype(BF16)


def call(body, out_shapes, *args, scratch=()):
    return pl.pallas_call(
        body,
        out_shape=[pltpu.VMEM(shape, kind) for shape, kind in out_shapes],
        in_specs=[pl.BlockSpec(memory_space=pltpu.VMEM)] * len(args),
        out_specs=[pl.BlockSpec(memory_space=pltpu.VMEM)] * len(out_shapes),
        scratch_shapes=list(scratch),
        name=body.__name__,
    )(*[pltpu.with_memory_space_constraint(a, pltpu.VMEM) for a in args])


def exchange(pieces, axes):
    return lax.all_to_all(pieces, axes, 0, 0, tiled=True)


def from_everyone(value, axes):
    peers = lax.axis_size(axes)
    return exchange(jnp.broadcast_to(value[None], (peers, *value.shape)), axes)


def own_half(value, core):
    rows = value.shape[0] // 2
    return lax.dynamic_slice_in_dim(value, core * rows, rows, 0)


def half_sum(partial, core):
    both = lax.all_gather(partial, "c")
    mine = lax.dynamic_slice_in_dim(both, core * 32, 32, 1).astype(F32)
    pair = (mine[0] + mine[1]).astype(BF16)
    return jnp.sum(from_everyone(pair, ("y",)).astype(F32), axis=0)


def routing(route_ids, route_weight, own):
    rows = route_ids.shape[0]
    names = jnp.arange(32, dtype=jnp.int32)
    hit = route_ids[:, :, None] == names[None, None, :]
    named = jnp.any(hit, axis=1)
    weight = jnp.sum(jnp.where(hit, route_weight[:, :, None], 0.0), axis=1)
    r = lax.broadcasted_iota(jnp.int32, (rows, rows), 0)
    q = lax.broadcasted_iota(jnp.int32, (rows, rows), 1)
    before = ((r // 8 == q // 8) & (q < r)).astype(BF16)
    earlier = mm(before, named.astype(BF16))
    group = lax.broadcasted_iota(jnp.int32, (rows, 1), 0) // 8
    place = ((group % 16) * 2).astype(F32) + earlier
    place = jnp.where(named, place, 64.0).astype(BF16)
    x = lax.broadcasted_iota(jnp.int32, (32, 1024), 0)
    slot = lax.broadcasted_iota(jnp.int32, (32, 1024), 1)
    spread = (slot // 32 == x).astype(BF16)
    tall = lax.dot_general(spread, place, (((0,), (1,)), ((), ())), preferred_element_type=F32)
    down = (lax.broadcasted_iota(jnp.int32, (1024, 1), 0) % 32).astype(F32)
    forth = (tall == down).astype(BF16)
    mine = lax.dynamic_slice_in_dim(forth, own * 32, 32, 0).astype(F32)
    own_weight = lax.dynamic_slice_in_dim(weight, own, 1, 1).reshape(1, rows)
    scaled = mine * own_weight
    slot_weight = jnp.concatenate(
        [
            jnp.sum(scaled[:, :128], axis=1, keepdims=True),
            jnp.sum(scaled[:, 128:], axis=1, keepdims=True),
        ],
        axis=0,
    )
    return forth, jnp.broadcast_to(slot_weight, (64, 128))


def per_device(
    residual,
    norm_gain,
    query_weight,
    key_weight,
    value_weight,
    gate_weight,
    out_weight,
    prior_state,
    lengths,
    ffn_gain,
    expert_gate,
    expert_up,
    expert_down,
    route_ids,
    route_weight,
    dense_gate,
    dense_up,
    dense_down,
    mix_vector,
):
    own = lax.axis_index(EP)
    core = lax.axis_index("c")
    head = lax.axis_index("y") * 2 + core
    (terms,) = call(
        project_body,
        [((32, 8, 896), BF16)],
        residual.T,
        norm_gain[None, :],
        query_weight,
        key_weight,
        value_weight,
        gate_weight,
    )
    arrived = exchange(terms, EP)

    forth, slot_weight = routing(route_ids, route_weight, own)
    gain_here = lax.dynamic_slice_in_dim(ffn_gain, own * 64, 64, 0)
    gain_here = jnp.broadcast_to(gain_here[:, None], (64, 128))
    mix_block = jnp.pad(mix_vector[:, None], ((0, 0), (0, 127)))
    dense_in = jnp.concatenate([dense_gate, dense_up, mix_block], axis=1)
    residual_half = own_half(residual.T, core).astype(F32)
    inverse = 1.0 / 10000.0 ** jnp.linspace(0.0, 1.0, 64, dtype=F32)
    angles = lengths.astype(F32)[:, None] * inverse[None, :]
    cosine = jnp.cos(angles)
    sine = jnp.sin(angles)
    cosine = jnp.concatenate([cosine, cosine], axis=1)
    sine = jnp.concatenate([-sine, sine], axis=1)
    decay = 1.0 - jnp.exp2(-1.0 - 0.5 * head.astype(F32))
    decay_row = jnp.broadcast_to(decay[None, None], (1, VAL_DIM))
    (
        arrived,
        forth,
        slot_weight,
        gain_here,
        dense_in,
        residual_half,
        cosine,
        sine,
        decay_row,
    ) = lax.optimization_barrier(
        (
            arrived,
            forth,
            slot_weight,
            gain_here,
            dense_in,
            residual_half,
            cosine,
            sine,
            decay_row,
        )
    )
    gated, key_rot, values = call(
        retain_body,
        [((32, 8, VAL_DIM), BF16), ((8, KEY_DIM), F32), ((8, VAL_DIM), F32)],
        arrived,
        prior_state[:, 0],
        cosine,
        sine,
        decay_row,
    )
    new_state = decay * prior_state + key_rot[:, None, :, None] * values[:, None, None, :]

    heads = exchange(gated, EP).reshape(256, VAL_DIM)
    attn = dots(out_weight.T, heads, 1, 1).astype(BF16)
    after_half = (residual_half + half_sum(attn, core)).astype(BF16)
    after = lax.all_gather(after_half, "c", tiled=True)

    (sent,) = call(
        dispatch_body, [((32, 56, 128), BF16)], after, forth, gain_here, dense_in
    )
    inbox = exchange(sent, EP)
    (made,) = call(
        expert_body,
        [((32, 40, 128), BF16)],
        inbox,
        ffn_gain[None, :],
        expert_gate[0],
        expert_up[0],
        expert_down[0],
        slot_weight,
        scratch=(pltpu.VMEM((64, D), BF16),),
    )
    returned = exchange(made, EP)
    (branch,) = call(collect_body, [((64, 256), BF16)], returned, forth, dense_down.T)
    out_half = (after_half.astype(F32) + half_sum(branch, core)).astype(BF16)
    layer_out = lax.all_gather(out_half, "c", tiled=True).T
    return layer_out, new_state


def solution(mesh):
    fine = Mesh(mesh.devices.reshape(8, 4, 8, 2), ("z", "x", "y", "c"))
    tp = ("y", "c")
    placed = (
        P(None, EP),
        P(EP),
        P(EP, tp),
        P(EP, tp),
        P(EP, tp),
        P(EP, tp),
        P(tp, EP),
        P(EP, tp, None, None),
        P(EP),
        P(),
        P(EP, None, tp),
        P(EP, None, tp),
        P(EP, tp, None),
        P(),
        P(),
        P(EP, tp),
        P(EP, tp),
        P(tp, EP),
        P(EP),
    )
    return jax.shard_map(
        per_device,
        mesh=fine,
        in_specs=placed,
        out_specs=(P(None, EP), P(EP, tp, None, None)),
        check_vma=False,
    )
```

```python
import jax
import jax.numpy as jnp
from jax import lax
from jax.experimental import pallas as pl
from jax.experimental.pallas import tpu as pltpu
from jax.sharding import Mesh, PartitionSpec as P

D = 2048
KEY_DIM = 128
VAL_DIM = 256
EPS = 1e-06
LIMIT = 7.0
ALPHA = 1.702
F32 = jnp.float32
BF16 = jnp.bfloat16
EP = ("z", "x")


def mm(a, b):
    return jnp.dot(a, b, preferred_element_type=F32)


def dots(a, b, i, j):
    return lax.dot_general(a, b, (((i,), (j,)), ((), ())), preferred_element_type=F32)


def two_part(v):
    high = v.astype(BF16).astype(F32)
    return high, v - high


def lane_of(shape):
    return lax.broadcasted_iota(jnp.int32, shape, len(shape) - 1)


def project_body(res_ref, gain_ref, q_ref, k_ref, v_ref, g_ref, out_ref):
    rows = res_ref[...].astype(F32).T
    normed = (rows * gain_ref[...]).astype(BF16)
    at = 0
    for ref in (q_ref, k_ref, v_ref, g_ref):
        width = ref.shape[1]
        part = mm(normed, ref[...])
        out_ref[:, :, at : at + width] = part.reshape(32, 8, width).astype(BF16)
        at += width
    high, low = two_part(jnp.sum(rows * rows, axis=1, keepdims=True))
    lane = lane_of((256, 128))
    stats = jnp.where(lane == 0, high, jnp.where(lane == 1, low, 0.0))
    out_ref[:, :, at : at + 128] = stats.reshape(32, 8, 128).astype(BF16)


def retain_body(arr_ref, prior_ref, cos_ref, sin_ref, decay_ref, out_ref, key_ref, value_ref):
    summed = jnp.sum(arr_ref[...].astype(F32), axis=0)
    scale = lax.rsqrt((summed[:, 768:769] + summed[:, 769:770]) / D + EPS)
    cosine = cos_ref[...]
    sine = sin_ref[...]
    query = summed[:, 0:128] * scale
    query = query * cosine + pltpu.roll(query, 64, 1) * sine
    key = summed[:, 128:256] * scale
    key = (key * cosine + pltpu.roll(key, 64, 1) * sine) * KEY_DIM ** (-0.5)
    value = summed[:, 256:512] * scale
    gate = summed[:, 512:768] * scale
    key_ref[...] = key
    value_ref[...] = value
    turned = query.T
    reads = [
        jnp.sum(turned[:, b : b + 1] * prior_ref[b], axis=0, keepdims=True) for b in range(8)
    ]
    met = jnp.sum(query * key, axis=1, keepdims=True)
    read = decay_ref[...] * jnp.concatenate(reads, axis=0) + met * value
    normed = read * lax.rsqrt(jnp.mean(read * read, axis=1, keepdims=True) + EPS)
    gated = normed * jax.nn.silu(gate)
    out_ref[...] = jnp.broadcast_to(gated[None], (32, 8, VAL_DIM)).astype(BF16)


def dispatch_body(am_ref, sel_ref, gain_ref, dense_ref, mix_ref, out_ref):
    am = am_ref[...].astype(F32)
    left = lane_of((64, 128)) < 64
    stacked = jnp.concatenate([jnp.where(left, am, 0.0), jnp.where(left, 0.0, am)], axis=0)
    sent = dots(sel_ref[...], stacked.astype(BF16), 1, 1)
    out_ref[:, 0:16, :] = sent.reshape(32, 16, 128).astype(BF16)
    normed = (am * gain_ref[:, 0:1]).astype(BF16)
    high, low = two_part(am * am)
    squares = jnp.concatenate([high, low], axis=0).astype(BF16)
    second = (lane_of((128, 128)) == 1).astype(F32).astype(BF16)
    stats = dots(normed, mix_ref[...], 0, 0) + dots(squares, second, 0, 0)
    high, low = two_part(stats)
    stats = (high + pltpu.roll(low, 2, 1)).reshape(16, 8, 128).astype(BF16)
    for half in range(2):
        at = 16 * half
        both = dots(normed, dense_ref[half, :, 0:256], 0, 0)
        out_ref[at : at + 16, 16:24, :] = both[:, :128].reshape(16, 8, 128).astype(BF16)
        out_ref[at : at + 16, 24:32, :] = both[:, 128:].reshape(16, 8, 128).astype(BF16)
        out_ref[at : at + 16, 32:40, :] = stats


def expert_body(
    arr_ref,
    gain_ref,
    eg_ref,
    eu_ref,
    pg_ref,
    pu_ref,
    weight_ref,
    ed_ref,
    pd_ref,
    out_ref,
    zn_ref,
    own_down,
    other_down,
    sems,
):
    first = pltpu.make_async_copy(ed_ref, own_down, sems.at[0])
    second = pltpu.make_async_copy(pd_ref, other_down, sems.at[1])
    first.start()
    second.start()
    tail = jnp.sum(arr_ref[:, 16:40, :].astype(F32), axis=0)
    stats = tail[16:24]
    scale = lax.rsqrt((stats[:, 1:2] + stats[:, 3:4]) / D + EPS)
    mix = jax.nn.sigmoid(scale * (stats[:, 0:1] + stats[:, 2:3]))
    act = jax.nn.silu(tail[0:8] * scale) * (tail[8:16] * scale) * mix
    out_ref[:, 16:24, :] = jnp.broadcast_to(act[None], (32, 8, 128)).astype(BF16)
    left = lane_of((16, 128)) < 64
    squares = jnp.zeros((32, 128), F32)
    for p in range(16):
        a = arr_ref[2 * p, 0:16, :].astype(F32)
        b = arr_ref[2 * p + 1, 0:16, :].astype(F32)
        z = jnp.concatenate(
            [
                jnp.where(left, a, pltpu.roll(b, 64, 1)),
                jnp.where(left, pltpu.roll(a, 64, 1), b),
            ],
            axis=0,
        )
        squares = squares + z * z
        zn_ref[:, 128 * p : 128 * p + 128] = (
            z * gain_ref[:, 128 * p : 128 * p + 128]
        ).astype(BF16)
    norm = lax.rsqrt(jnp.sum(squares, axis=1, keepdims=True) / D + EPS)
    zn = zn_ref[...]

    def hidden_of(gate_w, up_w):
        gate = jnp.minimum(mm(zn, gate_w[...]) * norm, LIMIT)
        up = jnp.clip(mm(zn, up_w[...]) * norm, -LIMIT, LIMIT)
        return ((up + 1.0) * gate * jax.nn.sigmoid(ALPHA * gate)).astype(BF16)

    own = hidden_of(eg_ref, eu_ref)
    other = hidden_of(pg_ref, pu_ref)
    weight = weight_ref[...]
    first.wait()
    second.wait()
    for p in range(16):
        at = slice(128 * p, 128 * p + 128)
        o = (mm(own, own_down[:, at]) + mm(other, other_down[:, at])) * weight
        low, high = o[0:16], o[16:32]
        out_ref[2 * p, 0:16, :] = jnp.where(left, low, pltpu.roll(high, 64, 1)).astype(BF16)
        out_ref[2 * p + 1, 0:16, :] = jnp.where(left, pltpu.roll(low, 64, 1), high).astype(BF16)


def collect_body(arr_ref, sel_ref, dense_ref, out_ref):
    slots = arr_ref[:, 0:16, :].reshape(512, 128)
    both = dots(slots, sel_ref[...], 0, 0)
    routed = jnp.where(lane_of((64, 128)) < 64, both[:64], both[64:])
    act = arr_ref[:, 16:24, :].astype(F32).reshape(256, 128).astype(BF16)
    dense = dots(dense_ref[0, :, 256:384], act[:128], 1, 1)
    dense = dense + dots(dense_ref[1, :, 256:384], act[128:], 1, 1)
    out_ref[...] = (routed + dense).astype(BF16)


def call(body, out_shapes, *args, far=(), scratch=(), near=True):
    if near:
        args = [pltpu.with_memory_space_constraint(a, pltpu.VMEM) for a in args]
    inside = pl.BlockSpec(memory_space=pltpu.VMEM)
    outside = pl.BlockSpec(memory_space=pl.ANY)
    return pl.pallas_call(
        body,
        out_shape=[pltpu.VMEM(shape, kind) for shape, kind in out_shapes],
        in_specs=[inside] * len(args) + [outside] * len(far),
        out_specs=[inside] * len(out_shapes),
        scratch_shapes=list(scratch),
        name=body.__name__,
    )(*args, *far)


def exchange(pieces, axes):
    return lax.all_to_all(pieces, axes, 0, 0, tiled=True)


def from_everyone(value, axes):
    peers = lax.axis_size(axes)
    return exchange(jnp.broadcast_to(value[None], (peers, *value.shape)), axes)


def own_half(value, core, dim):
    size = value.shape[dim] // 2
    return lax.dynamic_slice_in_dim(value, core * size, size, dim)


def sum_over_y(partial):
    return jnp.sum(from_everyone(partial, ("y",)).astype(F32), axis=0)


def partner(value):
    return lax.ppermute(value, "c", [(0, 1), (1, 0)])


def routing(route_ids, route_weight, own, core):
    rows = route_ids.shape[0]
    names = jnp.arange(32, dtype=jnp.int32)
    hit = route_ids[:, :, None] == names[None, None, :]
    named = jnp.any(hit, axis=1)
    weight = jnp.sum(jnp.where(hit, route_weight[:, :, None], 0.0), axis=1)
    r = lax.broadcasted_iota(jnp.int32, (rows, rows), 0)
    q = lax.broadcasted_iota(jnp.int32, (rows, rows), 1)
    before = ((r // 8 == q // 8) & (q < r)).astype(BF16)
    earlier = mm(before, named.astype(BF16))
    group = lax.broadcasted_iota(jnp.int32, (rows, 1), 0) // 8
    place = ((group % 8) * 2).astype(F32) + earlier
    place = own_half(jnp.where(named, place, 64.0).astype(BF16), core, 0)
    x = lax.broadcasted_iota(jnp.int32, (32, 512), 0)
    slot = lax.broadcasted_iota(jnp.int32, (32, 512), 1)
    spread = (slot // 16 == x).astype(BF16)
    tall = dots(spread, place, 0, 1)
    down = (lax.broadcasted_iota(jnp.int32, (512, 1), 0) % 16).astype(F32)
    select = (tall == down).astype(BF16)
    mine = lax.dynamic_slice_in_dim(select, own * 16, 16, 0).astype(F32)
    own_weight = lax.dynamic_slice_in_dim(own_half(weight, core, 0), own, 1, 1).reshape(1, 128)
    scaled = mine * own_weight
    slot_weight = jnp.concatenate(
        [
            jnp.sum(scaled[:, :64], axis=1, keepdims=True),
            jnp.sum(scaled[:, 64:], axis=1, keepdims=True),
        ],
        axis=0,
    )
    return select, jnp.broadcast_to(slot_weight, (32, 128))


def per_device(
    residual,
    norm_gain,
    query_weight,
    key_weight,
    value_weight,
    gate_weight,
    out_weight,
    prior_state,
    lengths,
    ffn_gain,
    expert_gate,
    expert_up,
    expert_down,
    route_ids,
    route_weight,
    dense_gate,
    dense_up,
    dense_down,
    mix_vector,
):
    own = lax.axis_index(EP)
    core = lax.axis_index("c")
    head = lax.axis_index("y") * 2 + core
    (terms,) = call(
        project_body,
        [((32, 8, 896), BF16)],
        residual.T,
        norm_gain[None, :],
        query_weight,
        key_weight,
        value_weight,
        gate_weight,
        near=False,
    )
    arrived = exchange(terms, EP)

    select, slot_weight = routing(route_ids, route_weight, own, core)
    gain_here = lax.dynamic_slice_in_dim(ffn_gain, own * 64, 64, 0)
    gain_here = jnp.broadcast_to(gain_here[:, None], (64, 128))
    mix_block = jnp.pad(mix_vector[:, None], ((0, 0), (0, 127)))
    dense = jnp.concatenate([dense_gate, dense_up, dense_down.T], axis=1)
    dense = lax.all_gather(dense, "c")
    other_gate = partner(expert_gate[0])
    residual_half = own_half(residual.T, core, 1).astype(F32)
    inverse = 1.0 / 10000.0 ** jnp.linspace(0.0, 1.0, 64, dtype=F32)
    angles = lengths.astype(F32)[:, None] * inverse[None, :]
    cosine = jnp.cos(angles)
    sine = jnp.sin(angles)
    cosine = jnp.concatenate([cosine, cosine], axis=1)
    sine = jnp.concatenate([-sine, sine], axis=1)
    decay = 1.0 - jnp.exp2(-1.0 - 0.5 * head.astype(F32))
    decay_row = jnp.broadcast_to(decay[None, None], (1, VAL_DIM))
    (
        arrived,
        select,
        slot_weight,
        gain_here,
        mix_block,
        dense,
        other_gate,
        residual_half,
        cosine,
        sine,
        decay_row,
    ) = lax.optimization_barrier(
        (
            arrived,
            select,
            slot_weight,
            gain_here,
            mix_block,
            dense,
            other_gate,
            residual_half,
            cosine,
            sine,
            decay_row,
        )
    )
    gated, key_rot, values = call(
        retain_body,
        [((32, 8, VAL_DIM), BF16), ((8, KEY_DIM), F32), ((8, VAL_DIM), F32)],
        arrived,
        prior_state[:, 0],
        cosine,
        sine,
        decay_row,
    )
    heads = exchange(gated, EP).reshape(256, VAL_DIM)

    new_state = decay * prior_state + key_rot[:, None, :, None] * values[:, None, None, :]
    other_up, other_down, _ = lax.optimization_barrier((expert_up[0], expert_down[0], cosine))
    other_up = partner(other_up)
    other_down = partner(other_down)
    heads, new_state, other_up, other_down = lax.optimization_barrier(
        (heads, new_state, other_up, other_down)
    )

    attn = dots(out_weight.T, heads, 1, 1).astype(BF16)
    pair = own_half(lax.all_gather(attn, "c"), core, 2).astype(F32)
    after_half = (residual_half + sum_over_y((pair[0] + pair[1]).astype(BF16))).astype(BF16)
    (sent,) = call(
        dispatch_body,
        [((32, 40, 128), BF16)],
        after_half,
        select,
        gain_here,
        dense,
        mix_block,
    )
    inbox = exchange(sent, EP)
    (made,) = call(
        expert_body,
        [((32, 24, 128), BF16)],
        inbox,
        ffn_gain[None, :],
        expert_gate[0],
        expert_up[0],
        other_gate,
        other_up,
        slot_weight,
        far=(expert_down[0], other_down),
        scratch=(
            pltpu.VMEM((32, D), BF16),
            pltpu.VMEM((128, D), BF16),
            pltpu.VMEM((128, D), BF16),
            pltpu.SemaphoreType.DMA((2,)),
        ),
    )
    returned = exchange(made, EP)
    (branch,) = call(collect_body, [((64, 128), BF16)], returned, select, dense)
    out_half = (after_half.astype(F32) + sum_over_y(branch)).astype(BF16)
    layer_out = lax.all_gather(out_half, "c")
    layer_out = jnp.transpose(layer_out, (0, 2, 1)).reshape(256, 64)
    return layer_out, new_state


def solution(mesh):
    fine = Mesh(mesh.devices.reshape(8, 4, 8, 2), ("z", "x", "y", "c"))
    tp = ("y", "c")
    placed = (
        P(None, EP),
        P(EP),
        P(EP, tp),
        P(EP, tp),
        P(EP, tp),
        P(EP, tp),
        P(tp, EP),
        P(EP, tp, None, None),
        P(EP),
        P(),
        P(EP, None, tp),
        P(EP, None, tp),
        P(EP, tp, None),
        P(),
        P(),
        P(EP, tp),
        P(EP, tp),
        P(tp, EP),
        P(EP),
    )
    return jax.shard_map(
        per_device,
        mesh=fine,
        in_specs=placed,
        out_specs=(P(None, EP), P(EP, tp, None, None)),
        check_vma=False,
    )
```

```python
import jax
import jax.numpy as jnp
from jax import lax
from jax.experimental import pallas as pl
from jax.experimental.pallas import tpu as pltpu
from jax.sharding import Mesh, PartitionSpec as P


D = 2048
KEY_DIM = 128
VAL_DIM = 256
EPS = 1e-06
LIMIT = 7.0
ALPHA = 1.702
F32 = jnp.float32
BF16 = jnp.bfloat16
EP = ("z", "x")


def mm(a, b):
    return jnp.dot(a, b, preferred_element_type=F32)


def dots(a, b, i, j):
    return lax.dot_general(a, b, (((i,), (j,)), ((), ())), preferred_element_type=F32)


def two_part(v):
    high = v.astype(BF16).astype(F32)
    return high, v - high


def lane_of(shape):
    return lax.broadcasted_iota(jnp.int32, shape, len(shape) - 1)


def project_body(res_ref, gain_ref, q_ref, k_ref, v_ref, g_ref, out_ref):
    rows = res_ref[...].astype(F32).T
    normed = (rows * gain_ref[...]).astype(BF16)
    at = 0
    for ref in (q_ref, k_ref, v_ref, g_ref):
        width = ref.shape[1]
        part = mm(normed, ref[...])
        out_ref[:, :, at : at + width] = part.reshape(32, 8, width).astype(BF16)
        at += width
    high, low = two_part(jnp.sum(rows * rows, axis=1, keepdims=True))
    lane = lane_of((256, 128))
    stats = jnp.where(lane == 0, high, jnp.where(lane == 1, low, 0.0))
    out_ref[:, :, at : at + 128] = stats.reshape(32, 8, 128).astype(BF16)


def retain_body(arr_ref, prior_ref, cos_ref, sin_ref, decay_ref, out_ref, key_ref, value_ref):
    summed = jnp.sum(arr_ref[...].astype(F32), axis=0)
    scale = lax.rsqrt((summed[:, 768:769] + summed[:, 769:770]) / D + EPS)
    cosine = cos_ref[...]
    sine = sin_ref[...]
    query = summed[:, 0:128] * scale
    query = query * cosine + pltpu.roll(query, 64, 1) * sine
    key = summed[:, 128:256] * scale
    key = (key * cosine + pltpu.roll(key, 64, 1) * sine) * KEY_DIM ** (-0.5)
    value = summed[:, 256:512] * scale
    gate = summed[:, 512:768] * scale
    key_ref[...] = key
    value_ref[...] = value
    turned = query.T
    reads = [
        jnp.sum(turned[:, b : b + 1] * prior_ref[b], axis=0, keepdims=True) for b in range(8)
    ]
    met = jnp.sum(query * key, axis=1, keepdims=True)
    read = decay_ref[...] * jnp.concatenate(reads, axis=0) + met * value
    normed = read * lax.rsqrt(jnp.mean(read * read, axis=1, keepdims=True) + EPS)
    gated = normed * jax.nn.silu(gate)
    out_ref[...] = jnp.broadcast_to(gated[None], (32, 8, VAL_DIM)).astype(BF16)


def dispatch_body(am_ref, sel_ref, gain_ref, dense_ref, mix_ref, out_ref):
    am = am_ref[...].astype(F32)
    left = lane_of((64, 128)) < 64
    stacked = jnp.concatenate([jnp.where(left, am, 0.0), jnp.where(left, 0.0, am)], axis=0)
    sent = dots(sel_ref[...], stacked.astype(BF16), 1, 1)
    out_ref[:, 0:16, :] = sent.reshape(32, 16, 128).astype(BF16)
    normed = (am * gain_ref[:, 0:1]).astype(BF16)
    high, low = two_part(am * am)
    squares = jnp.concatenate([high, low], axis=0).astype(BF16)
    second = (lane_of((128, 128)) == 1).astype(F32).astype(BF16)
    stats = dots(normed, mix_ref[...], 0, 0) + dots(squares, second, 0, 0)
    high, low = two_part(stats)
    stats = (high + pltpu.roll(low, 2, 1)).reshape(16, 8, 128).astype(BF16)
    for half in range(2):
        at = 16 * half
        both = dots(normed, dense_ref[half, :, 0:256], 0, 0)
        out_ref[at : at + 16, 16:24, :] = both[:, :128].reshape(16, 8, 128).astype(BF16)
        out_ref[at : at + 16, 24:32, :] = both[:, 128:].reshape(16, 8, 128).astype(BF16)
        out_ref[at : at + 16, 32:40, :] = stats


def expert_body(
    arr_ref,
    gain_ref,
    eg_ref,
    eu_ref,
    weight_ref,
    pg_ref,
    pu_ref,
    ed_ref,
    pd_ref,
    out_ref,
    zn_ref,
    other_gate,
    other_up,
    own_down,
    other_down,
    sems,
):
    loads = [
        pltpu.make_async_copy(pg_ref, other_gate, sems.at[0]),
        pltpu.make_async_copy(pu_ref, other_up, sems.at[1]),
        pltpu.make_async_copy(ed_ref, own_down, sems.at[2]),
        pltpu.make_async_copy(pd_ref, other_down, sems.at[3]),
    ]
    for load in loads:
        load.start()
    tail = jnp.sum(arr_ref[:, 16:40, :].astype(F32), axis=0)
    stats = tail[16:24]
    scale = lax.rsqrt((stats[:, 1:2] + stats[:, 3:4]) / D + EPS)
    mix = jax.nn.sigmoid(scale * (stats[:, 0:1] + stats[:, 2:3]))
    act = jax.nn.silu(tail[0:8] * scale) * (tail[8:16] * scale) * mix
    out_ref[:, 16:24, :] = jnp.broadcast_to(act[None], (32, 8, 128)).astype(BF16)
    left = lane_of((16, 128)) < 64
    squares = jnp.zeros((32, 128), F32)
    for p in range(16):
        a = arr_ref[2 * p, 0:16, :].astype(F32)
        b = arr_ref[2 * p + 1, 0:16, :].astype(F32)
        z = jnp.concatenate(
            [
                jnp.where(left, a, pltpu.roll(b, 64, 1)),
                jnp.where(left, pltpu.roll(a, 64, 1), b),
            ],
            axis=0,
        )
        squares = squares + z * z
        zn_ref[:, 128 * p : 128 * p + 128] = (
            z * gain_ref[:, 128 * p : 128 * p + 128]
        ).astype(BF16)
    norm = lax.rsqrt(jnp.sum(squares, axis=1, keepdims=True) / D + EPS)
    zn = zn_ref[...]

    def hidden_of(gate_w, up_w):
        gate = jnp.minimum(mm(zn, gate_w[...]) * norm, LIMIT)
        up = jnp.clip(mm(zn, up_w[...]) * norm, -LIMIT, LIMIT)
        return ((up + 1.0) * gate * jax.nn.sigmoid(ALPHA * gate)).astype(BF16)

    own = hidden_of(eg_ref, eu_ref)
    loads[0].wait()
    loads[1].wait()
    other = hidden_of(other_gate, other_up)
    weight = weight_ref[...]
    loads[2].wait()
    loads[3].wait()
    for p in range(16):
        at = slice(128 * p, 128 * p + 128)
        o = (mm(own, own_down[:, at]) + mm(other, other_down[:, at])) * weight
        low, high = o[0:16], o[16:32]
        out_ref[2 * p, 0:16, :] = jnp.where(left, low, pltpu.roll(high, 64, 1)).astype(BF16)
        out_ref[2 * p + 1, 0:16, :] = jnp.where(left, pltpu.roll(low, 64, 1), high).astype(BF16)


def collect_body(arr_ref, sel_ref, dense_ref, out_ref):
    slots = arr_ref[:, 0:16, :].reshape(512, 128)
    both = dots(slots, sel_ref[...], 0, 0)
    routed = jnp.where(lane_of((64, 128)) < 64, both[:64], both[64:])
    act = arr_ref[:, 16:24, :].astype(F32).reshape(256, 128).astype(BF16)
    dense = dots(dense_ref[0, :, 256:384], act[:128], 1, 1)
    dense = dense + dots(dense_ref[1, :, 256:384], act[128:], 1, 1)
    out_ref[...] = (routed + dense).astype(BF16)


def call(body, out_shapes, *args, far=(), scratch=(), near=True):
    if near:
        args = [pltpu.with_memory_space_constraint(a, pltpu.VMEM) for a in args]
    inside = pl.BlockSpec(memory_space=pltpu.VMEM)
    outside = pl.BlockSpec(memory_space=pl.ANY)
    return pl.pallas_call(
        body,
        out_shape=[pltpu.VMEM(shape, kind) for shape, kind in out_shapes],
        in_specs=[inside] * len(args) + [outside] * len(far),
        out_specs=[inside] * len(out_shapes),
        scratch_shapes=list(scratch),
    )(*args, *far)


def exchange(pieces, axes):
    return lax.all_to_all(pieces, axes, 0, 0, tiled=True)


def from_everyone(value, axes):
    peers = lax.axis_size(axes)
    return exchange(jnp.broadcast_to(value[None], (peers, *value.shape)), axes)


def own_half(value, core, dim):
    size = value.shape[dim] // 2
    return lax.dynamic_slice_in_dim(value, core * size, size, dim)


def sum_over_y(partial):
    return jnp.sum(from_everyone(partial, ("y",)).astype(F32), axis=0)


def partner(value):
    return lax.ppermute(value, "c", [(0, 1), (1, 0)])


def routing(route_ids, route_weight, own, core):
    rows = route_ids.shape[0]
    names = jnp.arange(32, dtype=jnp.int32)
    hit = route_ids[:, :, None] == names[None, None, :]
    named = jnp.any(hit, axis=1)
    weight = jnp.sum(jnp.where(hit, route_weight[:, :, None], 0.0), axis=1)
    r = lax.broadcasted_iota(jnp.int32, (rows, rows), 0)
    q = lax.broadcasted_iota(jnp.int32, (rows, rows), 1)
    before = ((r // 8 == q // 8) & (q < r)).astype(BF16)
    earlier = mm(before, named.astype(BF16))
    group = lax.broadcasted_iota(jnp.int32, (rows, 1), 0) // 8
    place = ((group % 8) * 2).astype(F32) + earlier
    place = own_half(jnp.where(named, place, 64.0).astype(BF16), core, 0)
    x = lax.broadcasted_iota(jnp.int32, (32, 512), 0)
    slot = lax.broadcasted_iota(jnp.int32, (32, 512), 1)
    spread = (slot // 16 == x).astype(BF16)
    tall = dots(spread, place, 0, 1)
    down = (lax.broadcasted_iota(jnp.int32, (512, 1), 0) % 16).astype(F32)
    select = (tall == down).astype(BF16)
    mine = lax.dynamic_slice_in_dim(select, own * 16, 16, 0).astype(F32)
    own_weight = lax.dynamic_slice_in_dim(own_half(weight, core, 0), own, 1, 1).reshape(1, 128)
    scaled = mine * own_weight
    slot_weight = jnp.concatenate(
        [
            jnp.sum(scaled[:, :64], axis=1, keepdims=True),
            jnp.sum(scaled[:, 64:], axis=1, keepdims=True),
        ],
        axis=0,
    )
    return select, jnp.broadcast_to(slot_weight, (32, 128))


def per_device(
    residual,
    norm_gain,
    query_weight,
    key_weight,
    value_weight,
    gate_weight,
    out_weight,
    prior_state,
    lengths,
    ffn_gain,
    expert_gate,
    expert_up,
    expert_down,
    route_ids,
    route_weight,
    dense_gate,
    dense_up,
    dense_down,
    mix_vector,
):
    own = lax.axis_index(EP)
    core = lax.axis_index("c")
    head = lax.axis_index("y") * 2 + core
    (terms,) = call(
        project_body,
        [((32, 8, 896), BF16)],
        residual.T,
        norm_gain[None, :],
        query_weight,
        key_weight,
        value_weight,
        gate_weight,
        near=False,
    )
    arrived = exchange(terms, EP)

    select, slot_weight = routing(route_ids, route_weight, own, core)
    gain_here = lax.dynamic_slice_in_dim(ffn_gain, own * 64, 64, 0)
    gain_here = jnp.broadcast_to(gain_here[:, None], (64, 128))
    mix_block = jnp.pad(mix_vector[:, None], ((0, 0), (0, 127)))
    dense = jnp.concatenate([dense_gate, dense_up, dense_down.T], axis=1)
    dense = lax.all_gather(dense, "c")
    other_gate = partner(expert_gate[0])
    residual_half = own_half(residual.T, core, 1).astype(F32)
    inverse = 1.0 / 10000.0 ** jnp.linspace(0.0, 1.0, 64, dtype=F32)
    angles = lengths.astype(F32)[:, None] * inverse[None, :]
    cosine = jnp.cos(angles)
    sine = jnp.sin(angles)
    cosine = jnp.concatenate([cosine, cosine], axis=1)
    sine = jnp.concatenate([-sine, sine], axis=1)
    decay = 1.0 - jnp.exp2(-1.0 - 0.5 * head.astype(F32))
    decay_row = jnp.broadcast_to(decay[None, None], (1, VAL_DIM))
    (
        arrived,
        select,
        slot_weight,
        gain_here,
        mix_block,
        dense,
        other_gate,
        residual_half,
        cosine,
        sine,
        decay_row,
    ) = lax.optimization_barrier(
        (
            arrived,
            select,
            slot_weight,
            gain_here,
            mix_block,
            dense,
            other_gate,
            residual_half,
            cosine,
            sine,
            decay_row,
        )
    )
    gated, key_rot, values = call(
        retain_body,
        [((32, 8, VAL_DIM), BF16), ((8, KEY_DIM), F32), ((8, VAL_DIM), F32)],
        arrived,
        prior_state[:, 0],
        cosine,
        sine,
        decay_row,
    )
    heads = exchange(gated, EP)
    heads = heads.reshape(256, VAL_DIM)

    new_state = decay * prior_state + key_rot[:, None, :, None] * values[:, None, None, :]
    other_up = partner(expert_up[0])
    other_down = partner(expert_down[0])
    heads, new_state, other_up, other_down = lax.optimization_barrier(
        (heads, new_state, other_up, other_down)
    )

    attn = dots(out_weight.T, heads, 1, 1).astype(BF16)
    pair = own_half(lax.all_gather(attn, "c"), core, 2).astype(F32)
    after_half = (residual_half + sum_over_y((pair[0] + pair[1]).astype(BF16))).astype(BF16)
    (sent,) = call(
        dispatch_body,
        [((32, 40, 128), BF16)],
        after_half,
        select,
        gain_here,
        dense,
        mix_block,
    )
    inbox = exchange(sent, EP)
    (made,) = call(
        expert_body,
        [((32, 24, 128), BF16)],
        inbox,
        ffn_gain[None, :],
        expert_gate[0],
        expert_up[0],
        slot_weight,
        far=(other_gate, other_up, expert_down[0], other_down),
        scratch=(
            pltpu.VMEM((32, D), BF16),
            pltpu.VMEM((D, 128), BF16),
            pltpu.VMEM((D, 128), BF16),
            pltpu.VMEM((128, D), BF16),
            pltpu.VMEM((128, D), BF16),
            pltpu.SemaphoreType.DMA((4,)),
        ),
    )
    returned = exchange(made, EP)
    (branch,) = call(collect_body, [((64, 128), BF16)], returned, select, dense)
    out_half = (after_half.astype(F32) + sum_over_y(branch)).astype(BF16)
    layer_out = lax.all_gather(out_half, "c")
    layer_out = jnp.transpose(layer_out, (0, 2, 1)).reshape(256, 64)
    return layer_out, new_state


def solution(mesh):
    fine = Mesh(mesh.devices.reshape(8, 4, 8, 2), ("z", "x", "y", "c"))
    tp = ("y", "c")
    placed = (
        P(None, EP),
        P(EP),
        P(EP, tp),
        P(EP, tp),
        P(EP, tp),
        P(EP, tp),
        P(tp, EP),
        P(EP, tp, None, None),
        P(EP),
        P(),
        P(EP, None, tp),
        P(EP, None, tp),
        P(EP, tp, None),
        P(),
        P(),
        P(EP, tp),
        P(EP, tp),
        P(tp, EP),
        P(EP),
    )

    return jax.shard_map(
        per_device,
        mesh=fine,
        in_specs=placed,
        out_specs=(P(None, EP), P(EP, tp, None, None)),
        check_vma=False,
    )
```

```python
import jax
import jax.numpy as jnp
from jax import lax
from jax.experimental import pallas as pl
from jax.experimental.pallas import tpu as pltpu
from jax.sharding import Mesh, PartitionSpec as P


D = 2048
KEY_DIM = 128
VAL_DIM = 256
EPS = 1e-06
LIMIT = 7.0
ALPHA = 1.702
F32 = jnp.float32
BF16 = jnp.bfloat16
EP = ("z", "x")


def mm(a, b):
    return jnp.dot(a, b, preferred_element_type=F32)


def dots(a, b, i, j):
    return lax.dot_general(a, b, (((i,), (j,)), ((), ())), preferred_element_type=F32)


def two_part(v):
    high = v.astype(BF16).astype(F32)
    return high, v - high


def lane_of(shape):
    return lax.broadcasted_iota(jnp.int32, shape, len(shape) - 1)


def project_body(res_ref, gain_ref, q_ref, k_ref, v_ref, g_ref, out_ref):
    rows = res_ref[...].astype(F32).T
    normed = (rows * gain_ref[...]).astype(BF16)
    at = 0
    for ref in (q_ref, k_ref, v_ref, g_ref):
        width = ref.shape[1]
        part = mm(normed, ref[...])
        out_ref[:, :, at : at + width] = part.reshape(32, 8, width).astype(BF16)
        at += width
    high, low = two_part(jnp.sum(rows * rows, axis=1, keepdims=True))
    lane = lane_of((256, 128))
    stats = jnp.where(lane == 0, high, jnp.where(lane == 1, low, 0.0))
    out_ref[:, :, at : at + 128] = stats.reshape(32, 8, 128).astype(BF16)


def retain_body(arr_ref, prior_ref, cos_ref, sin_ref, decay_ref, out_ref, key_ref, value_ref):
    summed = jnp.sum(arr_ref[...].astype(F32), axis=0)
    scale = lax.rsqrt((summed[:, 768:769] + summed[:, 769:770]) / D + EPS)
    cosine = cos_ref[...]
    sine = sin_ref[...]
    query = summed[:, 0:128] * scale
    query = query * cosine + pltpu.roll(query, 64, 1) * sine
    key = summed[:, 128:256] * scale
    key = (key * cosine + pltpu.roll(key, 64, 1) * sine) * KEY_DIM ** (-0.5)
    value = summed[:, 256:512] * scale
    gate = summed[:, 512:768] * scale
    key_ref[...] = key
    value_ref[...] = value
    turned = query.T
    reads = [
        jnp.sum(turned[:, b : b + 1] * prior_ref[b], axis=0, keepdims=True) for b in range(8)
    ]
    met = jnp.sum(query * key, axis=1, keepdims=True)
    read = decay_ref[...] * jnp.concatenate(reads, axis=0) + met * value
    normed = read * lax.rsqrt(jnp.mean(read * read, axis=1, keepdims=True) + EPS)
    gated = normed * jax.nn.silu(gate)
    out_ref[...] = jnp.broadcast_to(gated[None], (32, 8, VAL_DIM)).astype(BF16)


def dispatch_body(am_ref, sel_ref, gain_ref, dense_ref, mix_ref, out_ref):
    am = am_ref[...].astype(F32)
    left = lane_of((64, 128)) < 64
    stacked = jnp.concatenate([jnp.where(left, am, 0.0), jnp.where(left, 0.0, am)], axis=0)
    sent = dots(sel_ref[...], stacked.astype(BF16), 1, 1)
    out_ref[:, 0:16, :] = sent.reshape(32, 16, 128).astype(BF16)
    normed = (am * gain_ref[:, 0:1]).astype(BF16)
    high, low = two_part(am * am)
    squares = jnp.concatenate([high, low], axis=0).astype(BF16)
    second = (lane_of((128, 128)) == 1).astype(F32).astype(BF16)
    stats = dots(normed, mix_ref[...], 0, 0) + dots(squares, second, 0, 0)
    high, low = two_part(stats)
    stats = (high + pltpu.roll(low, 2, 1)).reshape(16, 8, 128).astype(BF16)
    for half in range(2):
        at = 16 * half
        both = dots(normed, dense_ref[half, :, 0:256], 0, 0)
        out_ref[at : at + 16, 16:24, :] = both[:, :128].reshape(16, 8, 128).astype(BF16)
        out_ref[at : at + 16, 24:32, :] = both[:, 128:].reshape(16, 8, 128).astype(BF16)
        out_ref[at : at + 16, 32:40, :] = stats


def expert_body(
    arr_ref,
    gain_ref,
    own_ref,
    weight_ref,
    other_ref,
    ed_ref,
    pd_ref,
    out_ref,
    zn_ref,
    other_in,
    own_down,
    other_down,
    sems,
):
    loads = [
        pltpu.make_async_copy(other_ref, other_in, sems.at[0]),
        pltpu.make_async_copy(ed_ref, own_down, sems.at[1]),
        pltpu.make_async_copy(pd_ref, other_down, sems.at[2]),
    ]
    for load in loads:
        load.start()
    tail = jnp.sum(arr_ref[:, 16:40, :].astype(F32), axis=0)
    stats = tail[16:24]
    scale = lax.rsqrt((stats[:, 1:2] + stats[:, 3:4]) / D + EPS)
    mix = jax.nn.sigmoid(scale * (stats[:, 0:1] + stats[:, 2:3]))
    act = jax.nn.silu(tail[0:8] * scale) * (tail[8:16] * scale) * mix
    out_ref[:, 16:24, :] = jnp.broadcast_to(act[None], (32, 8, 128)).astype(BF16)
    left = lane_of((16, 128)) < 64
    squares = jnp.zeros((32, 128), F32)
    for p in range(16):
        a = arr_ref[2 * p, 0:16, :].astype(F32)
        b = arr_ref[2 * p + 1, 0:16, :].astype(F32)
        z = jnp.concatenate(
            [
                jnp.where(left, a, pltpu.roll(b, 64, 1)),
                jnp.where(left, pltpu.roll(a, 64, 1), b),
            ],
            axis=0,
        )
        squares = squares + z * z
        zn_ref[:, 128 * p : 128 * p + 128] = (
            z * gain_ref[:, 128 * p : 128 * p + 128]
        ).astype(BF16)
    norm = lax.rsqrt(jnp.sum(squares, axis=1, keepdims=True) / D + EPS)
    zn = zn_ref[...]

    def hidden_of(weights):
        both = mm(zn, weights[...]) * norm
        gate = jnp.minimum(both[:, :128], LIMIT)
        up = jnp.clip(both[:, 128:], -LIMIT, LIMIT)
        return ((up + 1.0) * gate * jax.nn.sigmoid(ALPHA * gate)).astype(BF16)

    own = hidden_of(own_ref)
    loads[0].wait()
    other = hidden_of(other_in)
    weight = weight_ref[...]
    loads[1].wait()
    loads[2].wait()
    for p in range(16):
        at = slice(128 * p, 128 * p + 128)
        o = (mm(own, own_down[:, at]) + mm(other, other_down[:, at])) * weight
        low, high = o[0:16], o[16:32]
        out_ref[2 * p, 0:16, :] = jnp.where(left, low, pltpu.roll(high, 64, 1)).astype(BF16)
        out_ref[2 * p + 1, 0:16, :] = jnp.where(left, pltpu.roll(low, 64, 1), high).astype(BF16)


def collect_body(arr_ref, sel_ref, dense_ref, out_ref):
    slots = arr_ref[:, 0:16, :].reshape(512, 128)
    both = dots(slots, sel_ref[...], 0, 0)
    routed = jnp.where(lane_of((64, 128)) < 64, both[:64], both[64:])
    act = arr_ref[:, 16:24, :].astype(F32).reshape(256, 128).astype(BF16)
    dense = dots(dense_ref[0, :, 256:384], act[:128], 1, 1)
    dense = dense + dots(dense_ref[1, :, 256:384], act[128:], 1, 1)
    out_ref[...] = (routed + dense).astype(BF16)


def call(body, out_shapes, *args, far=(), scratch=(), near=True):
    if near:
        args = [pltpu.with_memory_space_constraint(a, pltpu.VMEM) for a in args]
    inside = pl.BlockSpec(memory_space=pltpu.VMEM)
    outside = pl.BlockSpec(memory_space=pl.ANY)
    return pl.pallas_call(
        body,
        out_shape=[pltpu.VMEM(shape, kind) for shape, kind in out_shapes],
        in_specs=[inside] * len(args) + [outside] * len(far),
        out_specs=[inside] * len(out_shapes),
        scratch_shapes=list(scratch),
    )(*args, *far)


def exchange(pieces, axes):
    return lax.all_to_all(pieces, axes, 0, 0, tiled=True)


def from_everyone(value, axes):
    peers = lax.axis_size(axes)
    return exchange(jnp.broadcast_to(value[None], (peers, *value.shape)), axes)


def own_half(value, core, dim):
    size = value.shape[dim] // 2
    return lax.dynamic_slice_in_dim(value, core * size, size, dim)


def sum_over_y(partial):
    return jnp.sum(from_everyone(partial, ("y",)).astype(F32), axis=0)


def partner(value):
    return lax.ppermute(value, "c", [(0, 1), (1, 0)])


def routing(route_ids, route_weight, own, core):
    rows = route_ids.shape[0]
    names = jnp.arange(32, dtype=jnp.int32)
    hit = route_ids[:, :, None] == names[None, None, :]
    named = jnp.any(hit, axis=1)
    weight = jnp.sum(jnp.where(hit, route_weight[:, :, None], 0.0), axis=1)
    r = lax.broadcasted_iota(jnp.int32, (rows, rows), 0)
    q = lax.broadcasted_iota(jnp.int32, (rows, rows), 1)
    before = ((r // 8 == q // 8) & (q < r)).astype(BF16)
    earlier = mm(before, named.astype(BF16))
    group = lax.broadcasted_iota(jnp.int32, (rows, 1), 0) // 8
    place = ((group % 8) * 2).astype(F32) + earlier
    place = own_half(jnp.where(named, place, 64.0).astype(BF16), core, 0)
    x = lax.broadcasted_iota(jnp.int32, (32, 512), 0)
    slot = lax.broadcasted_iota(jnp.int32, (32, 512), 1)
    spread = (slot // 16 == x).astype(BF16)
    tall = dots(spread, place, 0, 1)
    down = (lax.broadcasted_iota(jnp.int32, (512, 1), 0) % 16).astype(F32)
    select = (tall == down).astype(BF16)
    mine = lax.dynamic_slice_in_dim(select, own * 16, 16, 0).astype(F32)
    own_weight = lax.dynamic_slice_in_dim(own_half(weight, core, 0), own, 1, 1).reshape(1, 128)
    scaled = mine * own_weight
    slot_weight = jnp.concatenate(
        [
            jnp.sum(scaled[:, :64], axis=1, keepdims=True),
            jnp.sum(scaled[:, 64:], axis=1, keepdims=True),
        ],
        axis=0,
    )
    return select, jnp.broadcast_to(slot_weight, (32, 128))


def per_device(
    residual,
    norm_gain,
    query_weight,
    key_weight,
    value_weight,
    gate_weight,
    out_weight,
    prior_state,
    lengths,
    ffn_gain,
    expert_gate,
    expert_up,
    expert_down,
    route_ids,
    route_weight,
    dense_gate,
    dense_up,
    dense_down,
    mix_vector,
):
    own = lax.axis_index(EP)
    core = lax.axis_index("c")
    head = lax.axis_index("y") * 2 + core
    (terms,) = call(
        project_body,
        [((32, 8, 896), BF16)],
        residual.T,
        norm_gain[None, :],
        query_weight,
        key_weight,
        value_weight,
        gate_weight,
        near=False,
    )
    arrived = exchange(terms, EP)

    select, slot_weight = routing(route_ids, route_weight, own, core)
    gain_here = lax.dynamic_slice_in_dim(ffn_gain, own * 64, 64, 0)
    gain_here = jnp.broadcast_to(gain_here[:, None], (64, 128))
    mix_block = jnp.pad(mix_vector[:, None], ((0, 0), (0, 127)))
    dense = jnp.concatenate([dense_gate, dense_up, dense_down.T], axis=1)
    dense = lax.all_gather(dense, "c")
    own_in = jnp.concatenate([expert_gate[0], expert_up[0]], axis=1)
    other_in = partner(own_in)
    residual_half = own_half(residual.T, core, 1).astype(F32)
    inverse = 1.0 / 10000.0 ** jnp.linspace(0.0, 1.0, 64, dtype=F32)
    angles = lengths.astype(F32)[:, None] * inverse[None, :]
    cosine = jnp.cos(angles)
    sine = jnp.sin(angles)
    cosine = jnp.concatenate([cosine, cosine], axis=1)
    sine = jnp.concatenate([-sine, sine], axis=1)
    decay = 1.0 - jnp.exp2(-1.0 - 0.5 * head.astype(F32))
    decay_row = jnp.broadcast_to(decay[None, None], (1, VAL_DIM))
    (
        arrived,
        select,
        slot_weight,
        gain_here,
        mix_block,
        dense,
        other_in,
        residual_half,
        cosine,
        sine,
        decay_row,
    ) = lax.optimization_barrier(
        (
            arrived,
            select,
            slot_weight,
            gain_here,
            mix_block,
            dense,
            other_in,
            residual_half,
            cosine,
            sine,
            decay_row,
        )
    )
    gated, key_rot, values = call(
        retain_body,
        [((32, 8, VAL_DIM), BF16), ((8, KEY_DIM), F32), ((8, VAL_DIM), F32)],
        arrived,
        prior_state[:, 0],
        cosine,
        sine,
        decay_row,
    )
    heads = exchange(gated, EP)
    heads = heads.reshape(256, VAL_DIM)

    new_state = decay * prior_state + key_rot[:, None, :, None] * values[:, None, None, :]
    other_down = partner(expert_down[0])
    heads, new_state, other_down = lax.optimization_barrier((heads, new_state, other_down))

    attn = dots(out_weight.T, heads, 1, 1).astype(BF16)
    pair = own_half(lax.all_gather(attn, "c"), core, 2).astype(F32)
    after_half = (residual_half + sum_over_y((pair[0] + pair[1]).astype(BF16))).astype(BF16)
    (sent,) = call(
        dispatch_body,
        [((32, 40, 128), BF16)],
        after_half,
        select,
        gain_here,
        dense,
        mix_block,
    )
    inbox = exchange(sent, EP)
    (made,) = call(
        expert_body,
        [((32, 24, 128), BF16)],
        inbox,
        ffn_gain[None, :],
        own_in,
        slot_weight,
        far=(other_in, expert_down[0], other_down),
        scratch=(
            pltpu.VMEM((32, D), BF16),
            pltpu.VMEM((D, 256), BF16),
            pltpu.VMEM((128, D), BF16),
            pltpu.VMEM((128, D), BF16),
            pltpu.SemaphoreType.DMA((3,)),
        ),
    )
    returned = exchange(made, EP)
    (branch,) = call(collect_body, [((64, 128), BF16)], returned, select, dense)
    out_half = (after_half.astype(F32) + sum_over_y(branch)).astype(BF16)
    layer_out = lax.all_gather(out_half, "c")
    layer_out = jnp.transpose(layer_out, (0, 2, 1)).reshape(256, 64)
    return layer_out, new_state


def solution(mesh):
    fine = Mesh(mesh.devices.reshape(8, 4, 8, 2), ("z", "x", "y", "c"))
    tp = ("y", "c")
    placed = (
        P(None, EP),
        P(EP),
        P(EP, tp),
        P(EP, tp),
        P(EP, tp),
        P(EP, tp),
        P(tp, EP),
        P(EP, tp, None, None),
        P(EP),
        P(),
        P(EP, None, tp),
        P(EP, None, tp),
        P(EP, tp, None),
        P(),
        P(),
        P(EP, tp),
        P(EP, tp),
        P(tp, EP),
        P(EP),
    )

    return jax.shard_map(
        per_device,
        mesh=fine,
        in_specs=placed,
        out_specs=(P(None, EP), P(EP, tp, None, None)),
        check_vma=False,
    )
```

```python
import jax
import jax.numpy as jnp
from jax import lax
from jax.experimental import pallas as pl
from jax.experimental.pallas import tpu as pltpu
from jax.sharding import Mesh, PartitionSpec as P


D = 2048
KEY_DIM = 128
VAL_DIM = 256
EPS = 1e-06
LIMIT = 7.0
ALPHA = 1.702
F32 = jnp.float32
BF16 = jnp.bfloat16
EP = ("z", "x")


def mm(a, b):
    return jnp.dot(a, b, preferred_element_type=F32)


def dots(a, b, i, j):
    return lax.dot_general(a, b, (((i,), (j,)), ((), ())), preferred_element_type=F32)


def two_part(v):
    high = v.astype(BF16).astype(F32)
    return high, v - high


def lane_of(shape):
    return lax.broadcasted_iota(jnp.int32, shape, len(shape) - 1)


def project_body(res_ref, gain_ref, q_ref, k_ref, v_ref, g_ref, out_ref):
    rows = res_ref[...].astype(F32).T
    normed = (rows * gain_ref[...]).astype(BF16)
    at = 0
    for ref in (q_ref, k_ref, v_ref, g_ref):
        width = ref.shape[1]
        part = mm(normed, ref[...])
        out_ref[:, :, at : at + width] = part.reshape(32, 8, width).astype(BF16)
        at += width
    high, low = two_part(jnp.sum(rows * rows, axis=1, keepdims=True))
    lane = lane_of((256, 128))
    stats = jnp.where(lane == 0, high, jnp.where(lane == 1, low, 0.0))
    out_ref[:, :, at : at + 128] = stats.reshape(32, 8, 128).astype(BF16)


def retain_body(arr_ref, prior_ref, cos_ref, sin_ref, decay_ref, out_ref, key_ref, value_ref):
    summed = jnp.sum(arr_ref[...].astype(F32), axis=0)
    scale = lax.rsqrt((summed[:, 768:769] + summed[:, 769:770]) / D + EPS)
    cosine = cos_ref[...]
    sine = sin_ref[...]
    query = summed[:, 0:128] * scale
    query = query * cosine + pltpu.roll(query, 64, 1) * sine
    key = summed[:, 128:256] * scale
    key = (key * cosine + pltpu.roll(key, 64, 1) * sine) * KEY_DIM ** (-0.5)
    value = summed[:, 256:512] * scale
    gate = summed[:, 512:768] * scale
    key_ref[...] = key
    value_ref[...] = value
    turned = query.T
    reads = [
        jnp.sum(turned[:, b : b + 1] * prior_ref[b], axis=0, keepdims=True) for b in range(8)
    ]
    met = jnp.sum(query * key, axis=1, keepdims=True)
    read = decay_ref[...] * jnp.concatenate(reads, axis=0) + met * value
    normed = read * lax.rsqrt(jnp.mean(read * read, axis=1, keepdims=True) + EPS)
    gated = normed * jax.nn.silu(gate)
    out_ref[...] = jnp.broadcast_to(gated[None], (32, 8, VAL_DIM)).astype(BF16)


def dispatch_body(
    arr_ref, res_ref, sel_ref, gain_ref, dense_ref, mix_ref, out_ref, after_ref
):
    after = res_ref[...] + jnp.sum(arr_ref[...].astype(F32), axis=0)
    after_ref[...] = after.astype(BF16)
    am = after.astype(BF16).astype(F32)
    left = lane_of((64, 128)) < 64
    stacked = jnp.concatenate([jnp.where(left, am, 0.0), jnp.where(left, 0.0, am)], axis=0)
    sent = dots(sel_ref[...], stacked.astype(BF16), 1, 1)
    out_ref[:, 0:16, :] = sent.reshape(32, 16, 128).astype(BF16)
    normed = (am * gain_ref[:, 0:1]).astype(BF16)
    high, low = two_part(am * am)
    squares = jnp.concatenate([high, low], axis=0).astype(BF16)
    second = (lane_of((128, 128)) == 1).astype(F32).astype(BF16)
    stats = dots(normed, mix_ref[...], 0, 0) + dots(squares, second, 0, 0)
    high, low = two_part(stats)
    stats = (high + pltpu.roll(low, 2, 1)).reshape(16, 8, 128).astype(BF16)
    for half in range(2):
        at = 16 * half
        both = dots(normed, dense_ref[half, :, 0:256], 0, 0)
        out_ref[at : at + 16, 16:24, :] = both[:, :128].reshape(16, 8, 128).astype(BF16)
        out_ref[at : at + 16, 24:32, :] = both[:, 128:].reshape(16, 8, 128).astype(BF16)
        out_ref[at : at + 16, 32:40, :] = stats


def expert_body(
    arr_ref,
    gain_ref,
    own_ref,
    weight_ref,
    other_ref,
    ed_ref,
    pd_ref,
    out_ref,
    zn_ref,
    other_in,
    down,
    sems,
):
    loads = [
        pltpu.make_async_copy(other_ref, other_in, sems.at[0]),
        pltpu.make_async_copy(ed_ref, down.at[pl.ds(0, 128)], sems.at[1]),
        pltpu.make_async_copy(pd_ref, down.at[pl.ds(128, 128)], sems.at[2]),
    ]
    for load in loads:
        load.start()
    tail = jnp.sum(arr_ref[:, 16:40, :].astype(F32), axis=0)
    stats = tail[16:24]
    scale = lax.rsqrt((stats[:, 1:2] + stats[:, 3:4]) / D + EPS)
    mix = jax.nn.sigmoid(scale * (stats[:, 0:1] + stats[:, 2:3]))
    act = jax.nn.silu(tail[0:8] * scale) * (tail[8:16] * scale) * mix
    out_ref[:, 16:24, :] = jnp.broadcast_to(act[None], (32, 8, 128)).astype(BF16)
    left = lane_of((16, 128)) < 64
    squares = jnp.zeros((32, 128), F32)
    for p in range(16):
        a = arr_ref[2 * p, 0:16, :].astype(F32)
        b = arr_ref[2 * p + 1, 0:16, :].astype(F32)
        z = jnp.concatenate(
            [
                jnp.where(left, a, pltpu.roll(b, 64, 1)),
                jnp.where(left, pltpu.roll(a, 64, 1), b),
            ],
            axis=0,
        )
        squares = squares + z * z
        zn_ref[:, 128 * p : 128 * p + 128] = (
            z * gain_ref[:, 128 * p : 128 * p + 128]
        ).astype(BF16)
    norm = lax.rsqrt(jnp.sum(squares, axis=1, keepdims=True) / D + EPS)
    zn = zn_ref[...]

    def hidden_of(weights):
        both = mm(zn, weights[...]) * norm
        gate = jnp.minimum(both[:, :128], LIMIT)
        up = jnp.clip(both[:, 128:], -LIMIT, LIMIT)
        return ((up + 1.0) * gate * jax.nn.sigmoid(ALPHA * gate)).astype(BF16)

    own = hidden_of(own_ref)
    loads[0].wait()
    other = hidden_of(other_in)
    weight = weight_ref[:, 0:1]
    loads[1].wait()
    loads[2].wait()
    hidden = jnp.concatenate([own, other], axis=1)
    for q in range(8):
        wide = mm(hidden, down[:, 256 * q : 256 * q + 256]) * weight
        for k in range(2):
            p = 2 * q + k
            o = wide[:, 128 * k : 128 * k + 128]
            low, high = o[0:16], o[16:32]
            out_ref[2 * p, 0:16, :] = jnp.where(left, low, pltpu.roll(high, 64, 1)).astype(BF16)
            out_ref[2 * p + 1, 0:16, :] = jnp.where(left, pltpu.roll(low, 64, 1), high).astype(
                BF16
            )


def pair_body(both_ref, first_ref, out_ref):
    both = both_ref[...].astype(F32)
    total = both[0] + both[1]
    mine = jnp.where(first_ref[...] > 0.0, total[:, :128], total[:, 128:])
    out_ref[...] = jnp.broadcast_to(mine[None], (8, 64, 128)).astype(BF16)


def finish_body(arr_ref, after_ref, out_ref):
    total = jnp.sum(arr_ref[...].astype(F32), axis=0)
    out_ref[...] = (after_ref[...].astype(F32) + total).astype(BF16)


def collect_body(arr_ref, sel_ref, dense_ref, out_ref):
    slots = arr_ref[:, 0:16, :].reshape(512, 128)
    both = dots(slots, sel_ref[...], 0, 0)
    routed = jnp.where(lane_of((64, 128)) < 64, both[:64], both[64:])
    act = arr_ref[:, 16:24, :].astype(F32).reshape(256, 128).astype(BF16)
    dense = dots(dense_ref[0, :, 256:384], act[:128], 1, 1)
    dense = dense + dots(dense_ref[1, :, 256:384], act[128:], 1, 1)
    out_ref[...] = jnp.broadcast_to((routed + dense)[None], (8, 64, 128)).astype(BF16)


def call(body, out_shapes, *args, far=(), scratch=(), near=True):
    if near:
        args = [pltpu.with_memory_space_constraint(a, pltpu.VMEM) for a in args]
    inside = pl.BlockSpec(memory_space=pltpu.VMEM)
    outside = pl.BlockSpec(memory_space=pl.ANY)
    return pl.pallas_call(
        body,
        out_shape=[pltpu.VMEM(shape, kind) for shape, kind in out_shapes],
        in_specs=[inside] * len(args) + [outside] * len(far),
        out_specs=[inside] * len(out_shapes),
        scratch_shapes=list(scratch),
    )(*args, *far)


def exchange(pieces, axes):
    return lax.all_to_all(pieces, axes, 0, 0, tiled=True)


def own_half(value, core, dim):
    size = value.shape[dim] // 2
    return lax.dynamic_slice_in_dim(value, core * size, size, dim)


def partner(value):
    return lax.ppermute(value, "c", [(0, 1), (1, 0)])


def routing(route_ids, route_weight, own, core):
    rows = route_ids.shape[0]
    names = jnp.arange(32, dtype=jnp.int32)
    hit = route_ids[:, :, None] == names[None, None, :]
    named = jnp.any(hit, axis=1)
    weight = jnp.sum(jnp.where(hit, route_weight[:, :, None], 0.0), axis=1)
    r = lax.broadcasted_iota(jnp.int32, (rows, rows), 0)
    q = lax.broadcasted_iota(jnp.int32, (rows, rows), 1)
    before = ((r // 8 == q // 8) & (q < r)).astype(BF16)
    earlier = mm(before, named.astype(BF16))
    group = lax.broadcasted_iota(jnp.int32, (rows, 1), 0) // 8
    place = ((group % 8) * 2).astype(F32) + earlier
    place = own_half(jnp.where(named, place, 64.0).astype(BF16), core, 0)
    x = lax.broadcasted_iota(jnp.int32, (32, 512), 0)
    slot = lax.broadcasted_iota(jnp.int32, (32, 512), 1)
    spread = (slot // 16 == x).astype(BF16)
    tall = dots(spread, place, 0, 1)
    down = (lax.broadcasted_iota(jnp.int32, (512, 1), 0) % 16).astype(F32)
    select = (tall == down).astype(BF16)
    mine = lax.dynamic_slice_in_dim(select, own * 16, 16, 0).astype(F32)
    own_weight = lax.dynamic_slice_in_dim(own_half(weight, core, 0), own, 1, 1).reshape(1, 128)
    scaled = mine * own_weight
    slot_weight = jnp.concatenate(
        [
            jnp.sum(scaled[:, :64], axis=1, keepdims=True),
            jnp.sum(scaled[:, 64:], axis=1, keepdims=True),
        ],
        axis=0,
    )
    return select, jnp.broadcast_to(slot_weight, (32, 128))


def per_device(
    residual,
    norm_gain,
    query_weight,
    key_weight,
    value_weight,
    gate_weight,
    out_weight,
    prior_state,
    lengths,
    ffn_gain,
    expert_gate,
    expert_up,
    expert_down,
    route_ids,
    route_weight,
    dense_gate,
    dense_up,
    dense_down,
    mix_vector,
):
    own = lax.axis_index(EP)
    core = lax.axis_index("c")
    head = lax.axis_index("y") * 2 + core
    (terms,) = call(
        project_body,
        [((32, 8, 896), BF16)],
        residual.T,
        norm_gain[None, :],
        query_weight,
        key_weight,
        value_weight,
        gate_weight,
        near=False,
    )
    arrived = exchange(terms, EP)

    select, slot_weight = routing(route_ids, route_weight, own, core)
    gain_here = lax.dynamic_slice_in_dim(ffn_gain, own * 64, 64, 0)
    gain_here = jnp.broadcast_to(gain_here[:, None], (64, 128))
    mix_block = jnp.pad(mix_vector[:, None], ((0, 0), (0, 127)))
    dense = jnp.concatenate([dense_gate, dense_up, dense_down.T], axis=1)
    dense = lax.all_gather(dense, "c")
    own_in = jnp.concatenate([expert_gate[0], expert_up[0]], axis=1)
    other_in = partner(own_in)
    residual_half = own_half(residual.T, core, 1).astype(F32)
    inverse = 1.0 / 10000.0 ** jnp.linspace(0.0, 1.0, 64, dtype=F32)
    angles = lengths.astype(F32)[:, None] * inverse[None, :]
    cosine = jnp.cos(angles)
    sine = jnp.sin(angles)
    cosine = jnp.concatenate([cosine, cosine], axis=1)
    sine = jnp.concatenate([-sine, sine], axis=1)
    first_core = jnp.broadcast_to((1 - core).astype(F32)[None, None], (1, 128))
    decay = 1.0 - jnp.exp2(-1.0 - 0.5 * head.astype(F32))
    decay_row = jnp.broadcast_to(decay[None, None], (1, VAL_DIM))
    (
        arrived,
        select,
        slot_weight,
        gain_here,
        mix_block,
        dense,
        other_in,
        residual_half,
        cosine,
        sine,
        decay_row,
        first_core,
    ) = lax.optimization_barrier(
        (
            arrived,
            select,
            slot_weight,
            gain_here,
            mix_block,
            dense,
            other_in,
            residual_half,
            cosine,
            sine,
            decay_row,
            first_core,
        )
    )
    gated, key_rot, values = call(
        retain_body,
        [((32, 8, VAL_DIM), BF16), ((8, KEY_DIM), F32), ((8, VAL_DIM), F32)],
        arrived,
        prior_state[:, 0],
        cosine,
        sine,
        decay_row,
    )
    heads = exchange(gated, EP)
    heads = heads.reshape(256, VAL_DIM)

    new_state = decay * prior_state + key_rot[:, None, :, None] * values[:, None, None, :]
    other_down = partner(expert_down[0])
    heads, new_state, other_down = lax.optimization_barrier((heads, new_state, other_down))

    attn = dots(out_weight.T, heads, 1, 1).astype(BF16)
    (pair,) = call(
        pair_body, [((8, 64, 128), BF16)], lax.all_gather(attn, "c"), first_core
    )
    pieces = exchange(pair, ("y",))
    sent, after_half = call(
        dispatch_body,
        [((32, 40, 128), BF16), ((64, 128), BF16)],
        pieces,
        residual_half,
        select,
        gain_here,
        dense,
        mix_block,
    )
    inbox = exchange(sent, EP)
    (made,) = call(
        expert_body,
        [((32, 24, 128), BF16)],
        inbox,
        ffn_gain[None, :],
        own_in,
        slot_weight,
        far=(other_in, expert_down[0], other_down),
        scratch=(
            pltpu.VMEM((32, D), BF16),
            pltpu.VMEM((D, 256), BF16),
            pltpu.VMEM((256, D), BF16),
            pltpu.SemaphoreType.DMA((3,)),
        ),
    )
    returned = exchange(made, EP)
    (branch,) = call(collect_body, [((8, 64, 128), BF16)], returned, select, dense)
    (out_half,) = call(
        finish_body, [((64, 128), BF16)], exchange(branch, ("y",)), after_half
    )
    layer_out = lax.all_gather(out_half, "c")
    layer_out = jnp.transpose(layer_out, (0, 2, 1)).reshape(256, 64)
    return layer_out, new_state


def solution(mesh):
    fine = Mesh(mesh.devices.reshape(8, 4, 8, 2), ("z", "x", "y", "c"))
    tp = ("y", "c")
    placed = (
        P(None, EP),
        P(EP),
        P(EP, tp),
        P(EP, tp),
        P(EP, tp),
        P(EP, tp),
        P(tp, EP),
        P(EP, tp, None, None),
        P(EP),
        P(),
        P(EP, None, tp),
        P(EP, None, tp),
        P(EP, tp, None),
        P(),
        P(),
        P(EP, tp),
        P(EP, tp),
        P(tp, EP),
        P(EP),
    )

    return jax.shard_map(
        per_device,
        mesh=fine,
        in_specs=placed,
        out_specs=(P(None, EP), P(EP, tp, None, None)),
        check_vma=False,
    )
```

```python
import jax
import jax.numpy as jnp
from jax import lax
from jax.experimental import pallas as pl
from jax.experimental.pallas import tpu as pltpu
from jax.sharding import Mesh, PartitionSpec as P


D = 2048
KEY_DIM = 128
VAL_DIM = 256
EPS = 1e-06
LIMIT = 7.0
ALPHA = 1.702
F32 = jnp.float32
BF16 = jnp.bfloat16
EP = ("z", "x")


def mm(a, b):
    return jnp.dot(a, b, preferred_element_type=F32)


def dots(a, b, i, j):
    return lax.dot_general(a, b, (((i,), (j,)), ((), ())), preferred_element_type=F32)


def two_part(v):
    high = v.astype(BF16).astype(F32)
    return high, v - high


def lane_of(shape):
    return lax.broadcasted_iota(jnp.int32, shape, len(shape) - 1)


def project_body(res_ref, gain_ref, q_ref, k_ref, v_ref, g_ref, out_ref):
    rows = res_ref[...].astype(F32).T
    normed = (rows * gain_ref[...]).astype(BF16)
    at = 0
    for ref in (q_ref, k_ref, v_ref, g_ref):
        width = ref.shape[1]
        part = mm(normed, ref[...])
        out_ref[:, :, at : at + width] = part.reshape(32, 8, width).astype(BF16)
        at += width
    high, low = two_part(jnp.sum(rows * rows, axis=1, keepdims=True))
    lane = lane_of((256, 128))
    stats = jnp.where(lane == 0, high, jnp.where(lane == 1, low, 0.0))
    out_ref[:, :, at : at + 128] = stats.reshape(32, 8, 128).astype(BF16)


def retain_body(arr_ref, prior_ref, cos_ref, sin_ref, decay_ref, out_ref, key_ref, value_ref):
    summed = jnp.sum(arr_ref[...].astype(F32), axis=0)
    scale = lax.rsqrt((summed[:, 768:769] + summed[:, 769:770]) / D + EPS)
    cosine = cos_ref[...]
    sine = sin_ref[...]
    query = summed[:, 0:128] * scale
    query = query * cosine + pltpu.roll(query, 64, 1) * sine
    key = summed[:, 128:256] * scale
    key = (key * cosine + pltpu.roll(key, 64, 1) * sine) * KEY_DIM ** (-0.5)
    value = summed[:, 256:512] * scale
    gate = summed[:, 512:768] * scale
    key_ref[...] = key
    value_ref[...] = value
    turned = query.T
    reads = [
        jnp.sum(turned[:, b : b + 1] * prior_ref[b], axis=0, keepdims=True) for b in range(8)
    ]
    met = jnp.sum(query * key, axis=1, keepdims=True)
    read = decay_ref[...] * jnp.concatenate(reads, axis=0) + met * value
    normed = read * lax.rsqrt(jnp.mean(read * read, axis=1, keepdims=True) + EPS)
    gated = normed * jax.nn.silu(gate)
    out_ref[...] = jnp.broadcast_to(gated[None], (32, 8, VAL_DIM)).astype(BF16)


def dispatch_body(
    arr_ref, res_ref, sel_ref, gain_ref, dense_ref, mix_ref, out_ref, after_ref
):
    after = res_ref[...] + jnp.sum(arr_ref[...].astype(F32), axis=0)
    after_ref[...] = after.astype(BF16)
    am = after.astype(BF16).astype(F32)
    left = lane_of((64, 128)) < 64
    stacked = jnp.concatenate([jnp.where(left, am, 0.0), jnp.where(left, 0.0, am)], axis=0)
    sent = dots(sel_ref[...], stacked.astype(BF16), 1, 1)
    out_ref[:, 0:16, :] = sent.reshape(32, 16, 128).astype(BF16)
    normed = (am * gain_ref[:, 0:1]).astype(BF16)
    high, low = two_part(am * am)
    squares = jnp.concatenate([high, low], axis=0).astype(BF16)
    second = (lane_of((128, 128)) == 1).astype(F32).astype(BF16)
    stats = dots(normed, mix_ref[...], 0, 0) + dots(squares, second, 0, 0)
    high, low = two_part(stats)
    stats = (high + pltpu.roll(low, 2, 1)).reshape(16, 8, 128).astype(BF16)
    for half in range(2):
        at = 16 * half
        both = dots(normed, dense_ref[half, :, 0:256], 0, 0)
        out_ref[at : at + 16, 16:24, :] = both[:, :128].reshape(16, 8, 128).astype(BF16)
        out_ref[at : at + 16, 24:32, :] = both[:, 128:].reshape(16, 8, 128).astype(BF16)
        out_ref[at : at + 16, 32:40, :] = stats


def expert_body(
    arr_ref,
    gain_ref,
    own_ref,
    weight_ref,
    other_ref,
    ed_ref,
    pd_ref,
    out_ref,
    zn_ref,
    other_in,
    down,
    sems,
):
    loads = [
        pltpu.make_async_copy(other_ref, other_in, sems.at[0]),
        pltpu.make_async_copy(ed_ref, down.at[pl.ds(0, 128)], sems.at[1]),
        pltpu.make_async_copy(pd_ref, down.at[pl.ds(128, 128)], sems.at[2]),
    ]
    for load in loads:
        load.start()
    tail = jnp.sum(arr_ref[:, 16:40, :].astype(F32), axis=0)
    stats = tail[16:24]
    scale = lax.rsqrt((stats[:, 1:2] + stats[:, 3:4]) / D + EPS)
    mix = jax.nn.sigmoid(scale * (stats[:, 0:1] + stats[:, 2:3]))
    act = jax.nn.silu(tail[0:8] * scale) * (tail[8:16] * scale) * mix
    out_ref[:, 16:24, :] = jnp.broadcast_to(act[None], (32, 8, 128)).astype(BF16)
    left = lane_of((16, 128)) < 64
    squares = jnp.zeros((32, 128), F32)
    for p in range(16):
        a = arr_ref[2 * p, 0:16, :].astype(F32)
        b = arr_ref[2 * p + 1, 0:16, :].astype(F32)
        z = jnp.concatenate(
            [
                jnp.where(left, a, pltpu.roll(b, 64, 1)),
                jnp.where(left, pltpu.roll(a, 64, 1), b),
            ],
            axis=0,
        )
        squares = squares + z * z
        zn_ref[:, 128 * p : 128 * p + 128] = (
            z * gain_ref[:, 128 * p : 128 * p + 128]
        ).astype(BF16)
    norm = lax.rsqrt(jnp.sum(squares, axis=1, keepdims=True) / D + EPS)
    zn = zn_ref[...]

    def hidden_of(weights):
        both = mm(zn, weights[...]) * norm
        gate = jnp.minimum(both[:, :128], LIMIT)
        up = jnp.clip(both[:, 128:], -LIMIT, LIMIT)
        return ((up + 1.0) * gate * jax.nn.sigmoid(ALPHA * gate)).astype(BF16)

    own = hidden_of(own_ref)
    loads[0].wait()
    other = hidden_of(other_in)
    weight = weight_ref[:, 0:1]
    loads[1].wait()
    loads[2].wait()
    hidden = jnp.concatenate([own, other], axis=1)
    for q in range(8):
        wide = mm(hidden, down[:, 256 * q : 256 * q + 256]) * weight
        for k in range(2):
            p = 2 * q + k
            o = wide[:, 128 * k : 128 * k + 128]
            low, high = o[0:16], o[16:32]
            out_ref[2 * p, 0:16, :] = jnp.where(left, low, pltpu.roll(high, 64, 1)).astype(BF16)
            out_ref[2 * p + 1, 0:16, :] = jnp.where(left, pltpu.roll(low, 64, 1), high).astype(
                BF16
            )


def collect_body(arr_ref, sel_ref, dense_ref, out_ref):
    slots = arr_ref[:, 0:16, :].reshape(512, 128)
    both = dots(slots, sel_ref[...], 0, 0)
    routed = jnp.where(lane_of((64, 128)) < 64, both[:64], both[64:])
    act = arr_ref[:, 16:24, :].astype(F32).reshape(256, 128).astype(BF16)
    dense = dots(dense_ref[0, :, 256:384], act[:128], 1, 1)
    dense = dense + dots(dense_ref[1, :, 256:384], act[128:], 1, 1)
    out_ref[...] = jnp.broadcast_to((routed + dense)[None], (8, 64, 128)).astype(BF16)


def call(body, out_shapes, *args, far=(), scratch=(), near=True):
    if near:
        args = [pltpu.with_memory_space_constraint(a, pltpu.VMEM) for a in args]
    inside = pl.BlockSpec(memory_space=pltpu.VMEM)
    outside = pl.BlockSpec(memory_space=pl.ANY)
    return pl.pallas_call(
        body,
        out_shape=[pltpu.VMEM(shape, kind) for shape, kind in out_shapes],
        in_specs=[inside] * len(args) + [outside] * len(far),
        out_specs=[inside] * len(out_shapes),
        scratch_shapes=list(scratch),
    )(*args, *far)


def exchange(pieces, axes):
    return lax.all_to_all(pieces, axes, 0, 0, tiled=True)


def from_everyone(value, axes):
    peers = lax.axis_size(axes)
    return exchange(jnp.broadcast_to(value[None], (peers, *value.shape)), axes)


def own_half(value, core, dim):
    size = value.shape[dim] // 2
    return lax.dynamic_slice_in_dim(value, core * size, size, dim)


def partner(value):
    return lax.ppermute(value, "c", [(0, 1), (1, 0)])


def routing(route_ids, route_weight, own, core):
    rows = route_ids.shape[0]
    names = jnp.arange(32, dtype=jnp.int32)
    hit = route_ids[:, :, None] == names[None, None, :]
    named = jnp.any(hit, axis=1)
    weight = jnp.sum(jnp.where(hit, route_weight[:, :, None], 0.0), axis=1)
    r = lax.broadcasted_iota(jnp.int32, (rows, rows), 0)
    q = lax.broadcasted_iota(jnp.int32, (rows, rows), 1)
    before = ((r // 8 == q // 8) & (q < r)).astype(BF16)
    earlier = mm(before, named.astype(BF16))
    group = lax.broadcasted_iota(jnp.int32, (rows, 1), 0) // 8
    place = ((group % 8) * 2).astype(F32) + earlier
    place = own_half(jnp.where(named, place, 64.0).astype(BF16), core, 0)
    x = lax.broadcasted_iota(jnp.int32, (32, 512), 0)
    slot = lax.broadcasted_iota(jnp.int32, (32, 512), 1)
    spread = (slot // 16 == x).astype(BF16)
    tall = dots(spread, place, 0, 1)
    down = (lax.broadcasted_iota(jnp.int32, (512, 1), 0) % 16).astype(F32)
    select = (tall == down).astype(BF16)
    mine = lax.dynamic_slice_in_dim(select, own * 16, 16, 0).astype(F32)
    own_weight = lax.dynamic_slice_in_dim(own_half(weight, core, 0), own, 1, 1).reshape(1, 128)
    scaled = mine * own_weight
    slot_weight = jnp.concatenate(
        [
            jnp.sum(scaled[:, :64], axis=1, keepdims=True),
            jnp.sum(scaled[:, 64:], axis=1, keepdims=True),
        ],
        axis=0,
    )
    return select, jnp.broadcast_to(slot_weight, (32, 128))


def per_device(
    residual,
    norm_gain,
    query_weight,
    key_weight,
    value_weight,
    gate_weight,
    out_weight,
    prior_state,
    lengths,
    ffn_gain,
    expert_gate,
    expert_up,
    expert_down,
    route_ids,
    route_weight,
    dense_gate,
    dense_up,
    dense_down,
    mix_vector,
):
    own = lax.axis_index(EP)
    core = lax.axis_index("c")
    head = lax.axis_index("y") * 2 + core
    (terms,) = call(
        project_body,
        [((32, 8, 896), BF16)],
        residual.T,
        norm_gain[None, :],
        query_weight,
        key_weight,
        value_weight,
        gate_weight,
        near=False,
    )
    arrived = exchange(terms, EP)

    select, slot_weight = routing(route_ids, route_weight, own, core)
    gain_here = lax.dynamic_slice_in_dim(ffn_gain, own * 64, 64, 0)
    gain_here = jnp.broadcast_to(gain_here[:, None], (64, 128))
    mix_block = jnp.pad(mix_vector[:, None], ((0, 0), (0, 127)))
    dense = jnp.concatenate([dense_gate, dense_up, dense_down.T], axis=1)
    dense = lax.all_gather(dense, "c")
    own_in = jnp.concatenate([expert_gate[0], expert_up[0]], axis=1)
    other_in = partner(own_in)
    other_down = partner(expert_down[0])
    residual_half = own_half(residual.T, core, 1).astype(F32)
    inverse = 1.0 / 10000.0 ** jnp.linspace(0.0, 1.0, 64, dtype=F32)
    angles = lengths.astype(F32)[:, None] * inverse[None, :]
    cosine = jnp.cos(angles)
    sine = jnp.sin(angles)
    cosine = jnp.concatenate([cosine, cosine], axis=1)
    sine = jnp.concatenate([-sine, sine], axis=1)
    decay = 1.0 - jnp.exp2(-1.0 - 0.5 * head.astype(F32))
    decay_row = jnp.broadcast_to(decay[None, None], (1, VAL_DIM))
    (
        arrived,
        select,
        slot_weight,
        gain_here,
        mix_block,
        dense,
        other_in,
        other_down,
        residual_half,
        cosine,
        sine,
        decay_row,
    ) = lax.optimization_barrier(
        (
            arrived,
            select,
            slot_weight,
            gain_here,
            mix_block,
            dense,
            other_in,
            other_down,
            residual_half,
            cosine,
            sine,
            decay_row,
        )
    )
    gated, key_rot, values = call(
        retain_body,
        [((32, 8, VAL_DIM), BF16), ((8, KEY_DIM), F32), ((8, VAL_DIM), F32)],
        arrived,
        prior_state[:, 0],
        cosine,
        sine,
        decay_row,
    )
    heads = exchange(gated, EP)
    heads = heads.reshape(256, VAL_DIM)

    new_state = decay * prior_state + key_rot[:, None, :, None] * values[:, None, None, :]
    heads, new_state = lax.optimization_barrier((heads, new_state))

    attn = dots(out_weight.T, heads, 1, 1).astype(BF16)
    pair = own_half(lax.all_gather(attn, "c"), core, 2).astype(F32)
    pieces = from_everyone((pair[0] + pair[1]).astype(BF16), ("y",))
    sent, after_half = call(
        dispatch_body,
        [((32, 40, 128), BF16), ((64, 128), BF16)],
        pieces,
        residual_half,
        select,
        gain_here,
        dense,
        mix_block,
    )
    inbox = exchange(sent, EP)
    (made,) = call(
        expert_body,
        [((32, 24, 128), BF16)],
        inbox,
        ffn_gain[None, :],
        own_in,
        slot_weight,
        far=(other_in, expert_down[0], other_down),
        scratch=(
            pltpu.VMEM((32, D), BF16),
            pltpu.VMEM((D, 256), BF16),
            pltpu.VMEM((256, D), BF16),
            pltpu.SemaphoreType.DMA((3,)),
        ),
    )
    returned = exchange(made, EP)
    (branch,) = call(collect_body, [((8, 64, 128), BF16)], returned, select, dense)
    total = jnp.sum(exchange(branch, ("y",)).astype(F32), axis=0)
    out_half = (after_half.astype(F32) + total).astype(BF16)
    layer_out = lax.all_gather(out_half, "c")
    layer_out = jnp.transpose(layer_out, (0, 2, 1)).reshape(256, 64)
    return layer_out, new_state


def solution(mesh):
    fine = Mesh(mesh.devices.reshape(8, 4, 8, 2), ("z", "x", "y", "c"))
    tp = ("y", "c")
    placed = (
        P(None, EP),
        P(EP),
        P(EP, tp),
        P(EP, tp),
        P(EP, tp),
        P(EP, tp),
        P(tp, EP),
        P(EP, tp, None, None),
        P(EP),
        P(),
        P(EP, None, tp),
        P(EP, None, tp),
        P(EP, tp, None),
        P(),
        P(),
        P(EP, tp),
        P(EP, tp),
        P(tp, EP),
        P(EP),
    )

    return jax.shard_map(
        per_device,
        mesh=fine,
        in_specs=placed,
        out_specs=(P(None, EP), P(EP, tp, None, None)),
        check_vma=False,
    )
```
